128 devices in a mesh: ep: 16 (over z, x), tp: 8 (over y, core).
Axes of the slice: x: 4, y: 4, z: 4, core: 2. Of those that a mesh axis runs over, the one named last changes fastest.
Arguments:
- mixer_rows: bfloat16 [4096, 4096], P('ep'), may hold values from -8 to 8, as said below
- mixer_gain: float32 [4096], replicated, may hold values from 0.1 to 1.9
- gate_proj: bfloat16 [4096, 4096], P(None, 'tp'), may hold values from -0.09375 to 0.09375
- input_proj: bfloat16 [4096, 4096], P(None, 'tp'), may hold values from -0.09375 to 0.09375
- conv_taps: float32 [4, 4096], P(None, 'tp'), may hold values from -2 to 2
- input_gates: bfloat16 [16, 256, 256], P('tp'), may hold values from -0.375 to 0.375
- decay_gates: bfloat16 [16, 256, 256], P('tp'), may hold values from -0.375 to 0.375
- decay_offset: float32 [4096], P('tp'), may hold values from 4.8 to 13, as said below
- out_proj: bfloat16 [4096, 4096], P('tp'), may hold values from -0.09375 to 0.09375
- mixer_scale: float32 [4096], replicated, may hold values from 0.1 to 1.9
- expert_rows: bfloat16 [4096, 4096], P('ep'), may hold values from -6 to 6
- expert_gain: float32 [4096], replicated, may hold values from 0.1 to 1.9
- route_ids: int32 [4096, 2], P('ep'), may hold values from 0 to 15, all different within a row; in each aligned block of 256 rows (0 to 255, 256 to 511, ...) at most 48 rows name the same one
- route_weights: float32 [4096, 2], P('ep'), may hold values from 0.5 to 2
- expert_gate: bfloat16 [16, 4096, 1024], P('ep', None, 'tp'), may hold values from -0.09375 to 0.09375
- expert_up: bfloat16 [16, 4096, 1024], P('ep', None, 'tp'), may hold values from -0.09375 to 0.09375
- expert_down: bfloat16 [16, 1024, 4096], P('ep', 'tp'), may hold values from -0.1875 to 0.1875
- shared_gate: bfloat16 [4096, 1024], P(None, 'tp'), may hold values from -0.09375 to 0.09375
- shared_up: bfloat16 [4096, 1024], P(None, 'tp'), may hold values from -0.09375 to 0.09375
- shared_down: bfloat16 [1024, 4096], P('tp'), may hold values from -0.1875 to 0.1875
- expert_scale: float32 [4096], replicated, may hold values from 0.1 to 1.9
Outputs:
- mixer_out: bfloat16 [4096, 4096], P(('ep', 'tp'))
- expert_out: bfloat16 [4096, 4096], P(('ep', 'tp'))
The draws below stay inside these ranges and needn't reach their ends.
Inputs may be any that keep to these rules, and one draw needn't show every extreme that they name: `mixer_rows`: order one, with a common direction whose weight drifts slowly along the sequence. `decay_offset`: the even channels forget within some 30 to 200 tokens; the odd channels keep 5 to 90 percent of their state over the whole sequence of 4096 tokens. `route_ids`: each row names 2 different experts; within the rows of one index of ep (aligned blocks of 256 rows) no expert is named by more than 48 rows, and in some blocks one is named by exactly 48.
All inputs are finite; a program needn't handle non-finite values.
Results may differ from the reference program's by a relative error of at most 0.0033.
The reference program's roundings to bfloat16 on the way count: a program that leaves them out, or rounds other values in their place, can miss the bound.
Values may be sent and summed in bfloat16 or wider, within the bound.
A program may use at most 192 MiB of HBM per device.

```python
import math
import jax
import jax.numpy as jnp
import numpy as np
from jax import lax

D = 4096
RNN_BLOCKS = 16
BLOCK_WIDTH = 256
CONV = 4
EXPERT_HIDDEN = 1024
SHARED_HIDDEN = 1024
TOP_K = 2
ROWS = 256
EXPERTS = 16
TOKENS = 4096
CAP = 48
N_EP = 16


def draw_mixer_rows(key, part):
    noise_key, direction_key, phase_key = jax.random.split(key, 3)
    noise_part = jax.random.normal(noise_key, (TOKENS, D), jnp.float32)
    direction = jax.random.normal(direction_key, (D,), jnp.float32)
    phase_shift = jax.random.uniform(phase_key, (), jnp.float32, 0.0, 2.0 * math.pi)
    positions = jnp.arange(TOKENS, dtype=jnp.float32) / TOKENS
    drift_level = 2.0 * jnp.sin(3.0 * math.pi * positions + phase_shift)
    values = noise_part + drift_level[:, None] * direction[None, :]
    return jnp.clip(values, -8.0, 8.0).astype(jnp.bfloat16)


def draw_decay_offset(key, part):
    fast_key, slow_key = jax.random.split(key)
    fast_part = jax.random.uniform(fast_key, (D,), jnp.float32, 4.8, 6.7)
    slow_part = math.log(TOKENS) + jax.random.uniform(slow_key, (D,), jnp.float32, 0.3, 3.6)
    parity = jnp.arange(D) % 2
    return jnp.where(parity == 0, fast_part, slow_part).astype(jnp.float32)


def levels(key, dims, pieces, least, high):
    gain = 1.0
    for axis_at, shards_of in pieces:
        heights = jax.random.uniform(jax.random.fold_in(jax.random.fold_in(key, 6), axis_at), (shards_of,), jnp.float32, least / len(pieces), high / len(pieces))
        gain = gain * jnp.repeat(jnp.exp(heights), dims[axis_at] // shards_of).reshape((-1,) + (1,) * (len(dims) - 1 - axis_at))
    return gain


def routed_block(key, own, number, rows, amount, top, most, skew):
    order = jax.random.permutation(key, amount)
    crowded, common = portions_of(amount, rows * top, most, skew, True), portions_of(amount, rows * top, most, skew, False)
    places = jnp.arange(amount)

    def named(lengths, offset_by):
        used = int((lengths > 0).sum())
        fixed = max(1, used // 4)
        shifted = fixed + (places - fixed + offset_by * (used - fixed)) % max(1, amount - fixed)
        return jnp.zeros((amount,), jnp.int32).at[order[jnp.where(places < fixed, places, shifted)]].set(jnp.asarray(lengths, jnp.int32))

    lengths = jnp.where(number % 4 == 0, named(crowded, number // 4), named(common, number - number // 4 - 1))
    mixed = jax.random.permutation(jax.random.fold_in(own, 3), amount)
    donor, sink = mixed[0:amount // 2 * 2:2], mixed[1:amount // 2 * 2:2]
    room = jnp.minimum(lengths[donor] - 1, most - lengths[sink]) // 2
    room = jnp.where((donor == order[0]) | (sink == order[0]) | (lengths[sink] == 0), 0, jnp.maximum(room, 0))
    shifted = jax.random.randint(jax.random.fold_in(own, 4), (amount // 2,), 0, 1 << 20) % (room + 1)
    lengths = lengths.at[donor].add(-shifted).at[sink].add(shifted)
    members = jnp.searchsorted(jnp.cumsum(lengths), jnp.arange(rows * top), side="right").astype(jnp.int32)
    listing = members.reshape(top, rows).T
    listing = listing[jax.random.permutation(jax.random.fold_in(own, 1), rows)]
    offset_by = jax.random.randint(jax.random.fold_in(own, 2), (rows, 1), 0, top)
    return jnp.take_along_axis(listing, (jnp.arange(top)[None, :] + offset_by) % top, axis=1)


def portions_of(amount, total, bound, slope, full):
    portions = [(1 << 20) // math.isqrt(standing ** slope) + 1 for standing in range(1, amount + 1)]
    largest = bound if full else min(bound, max(-(-total // amount), total * portions[0] // sum(portions)))
    least = 1 if total - largest >= amount - 1 else 0
    counts, spare = [largest] + [least] * (amount - 1), total - largest - least * (amount - 1)
    while spare > 0:
        free = [i for i in range(1, amount) if counts[i] < largest] or [i for i in range(1, amount) if counts[i] < bound]
        whole, budget = sum([portions[i] for i in free]), spare
        for i in free:
            more = min(bound - counts[i], max(1, budget * portions[i] // whole), spare)
            counts[i] = counts[i] + more
            spare = spare - more
    return np.array(counts)


def centred(stream_key, shape, deviation, reach, cuts=(), kind=jnp.bfloat16):
    array = jax.random.normal(stream_key, shape, jnp.float32) * deviation
    if len(cuts) > 0:
        array = levels(stream_key, shape, cuts, -0.22, 0.18) * array
    return jnp.clip(array, min=-reach, max=reach).astype(kind)


def setup_inputs(seed: int = 0) -> dict:
    keys = jax.random.split(jax.random.key(seed), 22)
    mixer_rows = draw_mixer_rows(jax.random.fold_in(keys[21], 71), 0)
    mixer_gain = jnp.clip(1.0 + 0.18 * jax.random.normal(keys[1], (D,), jnp.float32), 0.1, 1.9)
    gate_proj = centred(keys[2], (D, D), D ** -0.5, 0.09375, ((1, 8),))
    input_proj = centred(keys[3], (D, D), D ** -0.5, 0.09375, ((1, 8),))
    conv_taps = centred(keys[4], (CONV, D), 0.5, 2.0, ((1, 8),), jnp.float32)
    input_gates = centred(keys[5], (RNN_BLOCKS, BLOCK_WIDTH, BLOCK_WIDTH), BLOCK_WIDTH ** -0.5, 0.375, ((0, 8),))
    decay_gates = centred(keys[6], (RNN_BLOCKS, BLOCK_WIDTH, BLOCK_WIDTH), BLOCK_WIDTH ** -0.5, 0.375, ((0, 8),))
    decay_offset = draw_decay_offset(jax.random.fold_in(keys[21], 71), 0)
    out_proj = centred(keys[8], (D, D), D ** -0.5, 0.09375, ((0, 8),))
    mixer_scale = jnp.clip(1.0 + 0.18 * jax.random.normal(keys[9], (D,), jnp.float32), 0.1, 1.9)
    expert_rows = centred(keys[10], (TOKENS, D), 1.0, 6.0, ((0, 16),))
    expert_gain = jnp.clip(1.0 + 0.18 * jax.random.normal(keys[11], (D,), jnp.float32), 0.1, 1.9)
    route_ids_keys = jax.random.split(jax.random.fold_in(keys[12], 1), TOKENS // ROWS)
    route_ids_turns = jax.random.permutation(jax.random.fold_in(keys[12], 3), TOKENS // ROWS)
    route_ids = jax.vmap(lambda own, number: routed_block(jax.random.fold_in(keys[12], 2), own, number, ROWS, EXPERTS, TOP_K, CAP, 1))(route_ids_keys, route_ids_turns).reshape((TOKENS, TOP_K))
    route_weights = jnp.clip(0.5 + 1.5 * jax.random.uniform(keys[13], (TOKENS, TOP_K), jnp.float32) ** levels(keys[13], (TOKENS, TOP_K), ((0, 16),), -0.2, 0.2), 0.5, 2.0)
    expert_gate = centred(keys[14], (EXPERTS, D, EXPERT_HIDDEN), D ** -0.5, 0.09375, ((0, 16), (2, 8)))
    expert_up = centred(keys[15], (EXPERTS, D, EXPERT_HIDDEN), D ** -0.5, 0.09375, ((0, 16), (2, 8)))
    expert_down = centred(keys[16], (EXPERTS, EXPERT_HIDDEN, D), EXPERT_HIDDEN ** -0.5, 0.1875, ((0, 16), (1, 8)))
    shared_gate = centred(keys[17], (D, SHARED_HIDDEN), D ** -0.5, 0.09375, ((1, 8),))
    shared_up = centred(keys[18], (D, SHARED_HIDDEN), D ** -0.5, 0.09375, ((1, 8),))
    shared_down = centred(keys[19], (SHARED_HIDDEN, D), SHARED_HIDDEN ** -0.5, 0.1875, ((0, 8),))
    expert_scale = jnp.clip(1.0 + 0.18 * jax.random.normal(keys[20], (D,), jnp.float32), 0.1, 1.9)
    return dict(mixer_rows=mixer_rows, mixer_gain=mixer_gain, gate_proj=gate_proj, input_proj=input_proj, conv_taps=conv_taps, input_gates=input_gates, decay_gates=decay_gates, decay_offset=decay_offset, out_proj=out_proj, mixer_scale=mixer_scale, expert_rows=expert_rows, expert_gain=expert_gain, route_ids=route_ids, route_weights=route_weights, expert_gate=expert_gate, expert_up=expert_up, expert_down=expert_down, shared_gate=shared_gate, shared_up=shared_up, shared_down=shared_down, expert_scale=expert_scale)


eps = 1e-06
lru_power = 8.0

def rms_scale(values, scale):
    floats = values.astype(jnp.float32)
    return floats * lax.rsqrt(lax.optimization_barrier(jnp.mean(floats * floats, axis=-1, keepdims=True)) + eps) * scale

def linear_pair(earlier, later):
    return (earlier[0] * later[0], later[0] * earlier[1] + later[1])

def slot_table(route_ids, expert_count, capacity):
    id_list = route_ids.reshape(-1).astype(jnp.int32)
    indicator = (id_list[:, None] == jnp.arange(expert_count, dtype=jnp.int32)[None, :]).astype(jnp.int32)
    earlier_count = (jnp.cumsum(indicator, axis=0).astype(jnp.int32) - indicator).astype(jnp.int32)
    position = lax.optimization_barrier(jnp.sum(earlier_count * indicator, axis=1)).astype(jnp.int32)
    slot_ids = (id_list * capacity + position).astype(jnp.int32)
    matched = (slot_ids[None, :] == jnp.arange(expert_count * capacity, dtype=jnp.int32)[:, None]).astype(jnp.int32)
    source = lax.optimization_barrier(jnp.sum(matched * jnp.arange(id_list.shape[0], dtype=jnp.int32)[None, :], axis=1)).astype(jnp.int32)
    filled = lax.optimization_barrier(jnp.sum(matched, axis=1)) > 0
    return (slot_ids, source, filled)

def mixer_half(mixer_rows, mixer_gain, gate_proj, input_proj, conv_taps, input_gates, decay_gates, decay_offset, out_proj, mixer_scale):
    row_count = mixer_rows.shape[0]
    normed = rms_scale(mixer_rows, mixer_gain).astype(jnp.bfloat16)
    gate_branch = jax.nn.gelu(jnp.dot(normed, gate_proj, preferred_element_type=jnp.float32))
    branch = jnp.dot(normed, input_proj, preferred_element_type=jnp.float32).astype(jnp.bfloat16)
    tap_count = conv_taps.shape[0]
    padded = jnp.concatenate([jnp.zeros((tap_count - 1, branch.shape[1]), branch.dtype), branch], axis=0)
    conv_sum = conv_taps[0] * padded[0:row_count].astype(jnp.float32)
    for tap_index in range(1, tap_count):
        conv_sum = conv_sum + conv_taps[tap_index] * padded[tap_index:tap_index + row_count].astype(jnp.float32)
    conv_out = conv_sum.astype(jnp.bfloat16)
    block_rows = conv_out.astype(jnp.float32).reshape(row_count, input_gates.shape[0], input_gates.shape[1])
    input_gate = jax.nn.sigmoid(jnp.einsum('rbi,bij->rbj', block_rows, input_gates.astype(jnp.float32))).reshape(row_count, -1)
    decay_gate = jax.nn.sigmoid(jnp.einsum('rbi,bij->rbj', block_rows, decay_gates.astype(jnp.float32))).reshape(row_count, -1)
    log_decay = -lru_power * decay_gate * jax.nn.softplus(-decay_offset)
    positions = jnp.arange(row_count, dtype=jnp.int32)
    input_scale = jnp.where((positions == 0)[:, None], 1.0, jnp.sqrt(-jnp.expm1(2.0 * log_decay)))
    drive_term = input_scale * input_gate * conv_out.astype(jnp.float32)
    decay_product, states = lax.associative_scan(linear_pair, (jnp.exp(log_decay), drive_term), axis=0)
    gated_rows = (gate_branch * states).astype(jnp.bfloat16)
    mixer_sum = jnp.dot(gated_rows, out_proj, preferred_element_type=jnp.float32)
    return rms_scale(mixer_sum, mixer_scale).astype(jnp.bfloat16)

def expert_half(expert_rows, expert_gain, route_ids, route_weights, expert_gate, expert_up, expert_down, shared_gate, shared_up, shared_down, expert_scale):
    expert_normed = rms_scale(expert_rows, expert_gain).astype(jnp.bfloat16)
    expert_count = expert_gate.shape[0]
    top_count = route_ids.shape[1]
    row_width = expert_rows.shape[1]
    gate_whole = expert_gate.astype(jnp.float32)
    up_whole = expert_up.astype(jnp.float32)
    down_whole = expert_down.astype(jnp.float32)

    def one_block(inputs):
        block_rows, block_ids, block_weights = inputs
        slot_ids, source, filled = slot_table(block_ids, expert_count, CAP)
        outgoing = jnp.where(filled[:, None], block_rows[source // top_count], jnp.zeros((), block_rows.dtype))
        outgoing = outgoing.reshape(expert_count, CAP, row_width).astype(jnp.float32)
        gate_part = jnp.einsum('ecd,edf->ecf', outgoing, gate_whole)
        up_part = jnp.einsum('ecd,edf->ecf', outgoing, up_whole)
        copy_hidden = (jax.nn.silu(gate_part) * up_part).astype(jnp.bfloat16)
        results = jnp.einsum('ecf,efd->ecd', copy_hidden.astype(jnp.float32), down_whole)
        picked = results.reshape(expert_count * CAP, row_width)[slot_ids] * block_weights.reshape(-1, 1)
        return lax.optimization_barrier(jnp.sum(picked.reshape(ROWS, top_count, row_width), axis=1))
    routed = lax.map(one_block, (expert_normed.reshape(N_EP, ROWS, row_width), route_ids.reshape(N_EP, ROWS, top_count), route_weights.reshape(N_EP, ROWS, top_count)))
    routed = routed.reshape(expert_rows.shape[0], row_width)
    shared_hidden = (jax.nn.silu(jnp.dot(expert_normed, shared_gate, preferred_element_type=jnp.float32)) * jnp.dot(expert_normed, shared_up, preferred_element_type=jnp.float32)).astype(jnp.bfloat16)
    expert_sum = routed + jnp.dot(shared_hidden, shared_down, preferred_element_type=jnp.float32)
    return rms_scale(expert_sum, expert_scale).astype(jnp.bfloat16)

def reference(mixer_rows, mixer_gain, gate_proj, input_proj, conv_taps, input_gates, decay_gates, decay_offset, out_proj, mixer_scale, expert_rows, expert_gain, route_ids, route_weights, expert_gate, expert_up, expert_down, shared_gate, shared_up, shared_down, expert_scale):
    mixer_out = mixer_half(mixer_rows, mixer_gain, gate_proj, input_proj, conv_taps, input_gates, decay_gates, decay_offset, out_proj, mixer_scale)
    expert_out = expert_half(expert_rows, expert_gain, route_ids, route_weights, expert_gate, expert_up, expert_down, shared_gate, shared_up, shared_down, expert_scale)
    return (mixer_out, expert_out)
```

```python
import jax
import jax.numpy as jnp
from jax import lax
from jax.experimental import pallas as pl
from jax.experimental.pallas import tpu as pltpu
from jax.sharding import PartitionSpec as P

eps = 1e-06
lru_power = 8.0


def shifted(block, axis, distance):
    devices = range(lax.axis_size(axis))
    route = [(i - distance, i) for i in devices if i - distance in devices]
    return lax.ppermute(block, axis, route)


def rms_scale(values, scale):
    floats = values.astype(jnp.float32)
    return floats * lax.rsqrt(jnp.mean(floats * floats, axis=-1, keepdims=True) + eps) * scale


def linear_pair(earlier, later):
    return (earlier[0] * later[0], later[0] * earlier[1] + later[1])


def slots_of(route_ids, expert_count, capacity):
    named = [
        (route_ids[:, k : k + 1] == jnp.arange(expert_count, dtype=jnp.int32)[None, :])
        for k in range(2)
    ]
    either = jnp.logical_or(*named).astype(jnp.bfloat16)
    count = route_ids.shape[0]
    before = jnp.tril(jnp.ones((count, count), jnp.bfloat16), -1)
    place = jnp.dot(before, either, preferred_element_type=jnp.float32)
    return [
        route_ids[:, k : k + 1] * capacity
        + jnp.sum(jnp.where(named[k], place, 0.0), axis=1, keepdims=True).astype(jnp.int32)
        for k in range(2)
    ]


MESH = pl.DeviceIdType.MESH
NCH = 2
CW = 2048 // NCH


def remote(src, dst, send, recv, device):
    return pltpu.make_async_remote_copy(
        src_ref=src, dst_ref=dst, send_sem=send, recv_sem=recv, device_id=device, device_id_type=MESH
    )


def exchange_kernel(
    send_x, eg, eu, ed, sd, op, sh, acum, loc, gate, cm, whi, wlo, mscale, escale,
    out_m, out_e,
    rows, w_in, w_dn, s_dn, o_pr, sh2, gts, carries, acc, hid, res, back,
    m_part, m_recv, m_sum, m_other, e_part, e_recv, e_sum, e_other,
    d_s, d_r, f_s, f_r, c_s, c_r, p_s, p_r, l_s, r_s, r_r, ms_s, ms_r, es_s, es_r, x_s, x_r,
):
    p = lax.axis_index("ep")
    t = lax.axis_index("tp")
    y = t // 2
    c = t % 2
    o = 1 - c
    par = p % 2
    half = p // 2
    partner = (p, 2 * y + o)

    barrier = pltpu.get_barrier_semaphore()

    def greet(k, _):
        other = (p * 2 + c + k) % 32
        pl.semaphore_signal(
            barrier, inc=1, device_id=(other // 2, 2 * y + other % 2), device_id_type=MESH
        )
        return 0

    lax.fori_loop(1, 32, greet, 0)
    for k in range(1, 4):
        pl.semaphore_signal(
            barrier, inc=1, device_id=(p, 2 * ((y + k) % 4) + c), device_id_type=MESH
        )
    pl.semaphore_wait(barrier, 34)

    def dispatch(step, j):
        i = (half + step) % 8
        return remote(
            send_x.at[i, j], rows.at[(y + 2 * j) % 4, half], d_s.at[i, j], d_r.at[half, j],
            (2 * i + c, 2 * y + 1 - par),
        )

    def arrival(step, j):
        i = (half + 8 - step) % 8
        return i, remote(
            send_x.at[i, j], rows.at[(y + 2 * j) % 4, i], d_s.at[i, j], d_r.at[i, j], partner
        )

    def go(step, j):
        dispatch(step, j).start()
        return j

    lax.fori_loop(0, 8, go, 0)
    lax.fori_loop(0, 8, go, 1)

    def carry(k):
        return remote(
            cm, carries.at[k - 1], c_s.at[k - 1], c_r.at[k - 1], ((p + k) % 16, t)
        )

    def carry_go(k, _):
        carry(k).start()
        return 0

    lax.fori_loop(1, 16, carry_go, 0)

    wide = lambda at: pl.ds(pl.multiple_of(at * 2048, 2048), 2048)
    swaps = [
        remote(sh, sh2, p_s.at[0], p_r.at[0], partner),
        remote(op.at[:, wide(o)], o_pr.at[1], p_s.at[1], p_r.at[1], partner),
        remote(eg, w_in.at[:, 256:384], p_s.at[2], p_r.at[2], partner),
        remote(eu, w_in.at[:, 384:512], p_s.at[3], p_r.at[3], partner),
        remote(ed, w_dn.at[128:256], p_s.at[4], p_r.at[4], partner),
        remote(sd.at[:, wide(o)], s_dn.at[1], p_s.at[5], p_r.at[5], partner),
    ]
    owns = [
        pltpu.make_async_copy(op.at[:, wide(c)], o_pr.at[0], l_s.at[0]),
        pltpu.make_async_copy(eg, w_in.at[:, 0:128], l_s.at[1]),
        pltpu.make_async_copy(eu, w_in.at[:, 128:256], l_s.at[2]),
        pltpu.make_async_copy(ed, w_dn.at[0:128], l_s.at[3]),
        pltpu.make_async_copy(sd.at[:, wide(c)], s_dn.at[0], l_s.at[4]),
    ]
    for copy in swaps + owns:
        copy.start()

    def carry_in(k, _):
        carry(k).wait_recv()
        return 0

    lax.fori_loop(1, 16, carry_in, 0)

    def fold(n, state):
        k = 15 - n
        later = carries[k - 1]
        return jnp.where(k <= p, later[0:4] * state + later[4:8], state)

    state = lax.fori_loop(0, 15, fold, jnp.zeros((4, 128), jnp.float32))
    for j in range(4):
        cols = slice(128 * j, 128 * j + 128)
        states = loc[:, cols] + acum[:, cols] * state[j : j + 1]
        gts[0, :, cols] = (gate[:, cols] * states).astype(jnp.bfloat16)

    gswap = remote(gts.at[0], gts.at[1], p_s.at[6], p_r.at[6], partner)
    gswap.start()

    def forward(i, d):
        return remote(
            rows.at[y, i], rows.at[y, i], f_s.at[i, d], f_r.at[i, d],
            (p, 2 * ((y + 1 + 2 * d) % 4) + c),
        )

    def relay(step, _):
        i, copy = arrival(step, 0)
        copy.wait_recv()
        forward(i, 0).start()
        forward(i, 1).start()
        return 0

    lax.fori_loop(0, 8, relay, 0)

    def scatter(part, recv, send_sem, recv_sem, ch):
        return [
            remote(
                part.at[ch, (y + k) % 4], recv.at[ch, k - 1], send_sem.at[ch, k - 1],
                recv_sem.at[ch, k - 1], (p, 2 * ((y + k) % 4) + c),
            )
            for k in range(1, 4)
        ]

    def settle(part, recv, total, other, send_sem, recv_sem, base, ch):
        for copy in scatter(part, recv, send_sem, recv_sem, ch):
            copy.wait_recv()
        value = part[ch, y] + recv[ch, 0] + recv[ch, 1] + recv[ch, 2]
        total[ch] = value.reshape(2, 32, CW)
        swap(total, other, base, ch).start()

    def swap(total, other, base, ch):
        return remote(
            total.at[ch, o], other.at[ch], x_s.at[base + ch], x_r.at[base + ch], partner
        )

    def finish(total, other, scale, out, base):
        square = jnp.zeros((32, 1), jnp.float32)
        for ch in range(NCH):
            swap(total, other, base, ch).wait_recv()
            mine, theirs = total[ch, c], other[ch]
            square += jnp.sum(mine * mine + theirs * theirs, axis=1, keepdims=True)
        factor = lax.rsqrt(square / 4096.0 + eps)
        for ch in range(NCH):
            for values, side in ((total[ch, c], c), (other[ch], o)):
                cols = pl.ds(pl.multiple_of(side * 2048 + ch * CW, CW), CW)
                out[:, cols] = (values * factor * scale[:, cols]).astype(jnp.bfloat16)

    owns[0].wait()
    swaps[1].wait_recv()
    gswap.wait_recv()
    for ch in range(NCH):
        cols = slice(ch * CW, ch * CW + CW)
        m_part[ch] = (
            jnp.dot(gts[0], o_pr[0, :, cols], preferred_element_type=jnp.float32)
            + jnp.dot(gts[1], o_pr[1, :, cols], preferred_element_type=jnp.float32)
        ).reshape(4, 64, CW)
        for copy in scatter(m_part, m_recv, ms_s, ms_r, ch):
            copy.start()

    owns[4].wait()
    swaps[0].wait_recv()
    swaps[5].wait_recv()
    for ch in range(NCH):
        cols = slice(ch * CW, ch * CW + CW)
        e_part[ch] = (
            jnp.dot(sh[...], s_dn[0, :, cols], preferred_element_type=jnp.float32)
            + jnp.dot(sh2[...], s_dn[1, :, cols], preferred_element_type=jnp.float32)
        ).reshape(4, 64, CW)

    for copy in owns[1:4]:
        copy.wait()
    for copy in swaps[2:5]:
        copy.wait_recv()

    def landed(step, _):
        i, copy = arrival(step, 1)
        copy.wait_recv()
        for d in range(2):
            source = (y + 3 + 2 * d) % 4
            remote(
                rows.at[source, i], rows.at[source, i], f_s.at[i, d], f_r.at[i, d], partner
            ).wait_recv()
        return 0

    lax.fori_loop(0, 8, landed, 0)

    acc[...] = jnp.zeros_like(acc)

    def quarter(q, _):
        depth = pl.ds(pl.multiple_of(q * 1024, 1024), 1024)
        acc[...] += jnp.dot(
            rows[q].reshape(384, 1024), w_in[depth, :], preferred_element_type=jnp.float32
        )
        return 0

    lax.fori_loop(0, 4, quarter, 0)
    for side in range(2):
        g = acc[:, 256 * side : 256 * side + 128]
        u = acc[:, 256 * side + 128 : 256 * side + 256]
        hid[:, 128 * side : 128 * side + 128] = (
            g / (1.0 + jnp.exp(-g)) * u
        ).astype(jnp.bfloat16)

    def returning(ch, step, h):
        i = (half + step) % 8
        s = 2 * i + o
        return i, s, remote(
            res.at[ch, h, i], back.at[ch, p], r_s.at[ch, i, h], r_r.at[ch, p], (s, 2 * y + h)
        )

    def give(ch):
        for h in range(2):
            cols = slice(h * 2048 + ch * CW, h * 2048 + ch * CW + CW)
            res[ch, h] = (
                jnp.dot(hid[...], w_dn[:, cols], preferred_element_type=jnp.float32)
                .astype(jnp.bfloat16)
                .reshape(8, 48, CW)
            )

        def send(step, _):
            for h in range(2):
                i, s, copy = returning(ch, step, h)

                @pl.when(jnp.logical_or(s != p, c != h))
                def _():
                    copy.start()

                @pl.when(jnp.logical_and(s == p, c == h))
                def _():
                    back[ch, p] = res[ch, h, i]

            return 0

        lax.fori_loop(0, 8, send, 0)

    for ch in range(NCH):
        give(ch)

    for ch in range(NCH):
        settle(m_part, m_recv, m_sum, m_other, ms_s, ms_r, 0, ch)
    finish(m_sum, m_other, mscale, out_m, 0)

    for ch in range(NCH):

        def got(e, _):
            @pl.when(jnp.logical_or(e != p, c != 1 - par))
            def _():
                remote(
                    res.at[ch, 0, 0], back.at[ch, e], r_s.at[ch, 0, 0], r_r.at[ch, e], partner
                ).wait_recv()

            return 0

        lax.fori_loop(0, 16, got, 0)
        rows_back = back[ch].reshape(768, CW)
        e_part[ch] = e_part[ch] + (
            jnp.dot(whi[...], rows_back, preferred_element_type=jnp.float32)
            + jnp.dot(wlo[...], rows_back, preferred_element_type=jnp.float32)
        ).reshape(4, 64, CW)
        for copy in scatter(e_part, e_recv, es_s, es_r, ch):
            copy.start()

    for ch in range(NCH):
        settle(e_part, e_recv, e_sum, e_other, es_s, es_r, NCH, ch)
    finish(e_sum, e_other, escale, out_e, NCH)

    def drain(step, _):
        for j in range(2):
            dispatch(step, j).wait_send()
            forward(step, j).wait_send()
        for ch in range(NCH):
            for h in range(2):
                i, s, copy = returning(ch, step, h)

                @pl.when(jnp.logical_or(s != p, c != h))
                def _():
                    copy.wait_send()

        return 0

    lax.fori_loop(0, 8, drain, 0)

    def carry_out(k, _):
        carry(k).wait_send()
        return 0

    lax.fori_loop(1, 16, carry_out, 0)
    for copy in swaps:
        copy.wait_send()
    gswap.wait_send()
    for ch in range(NCH):
        for copy in scatter(m_part, m_recv, ms_s, ms_r, ch):
            copy.wait_send()
        for copy in scatter(e_part, e_recv, es_s, es_r, ch):
            copy.wait_send()
        swap(m_sum, m_other, 0, ch).wait_send()
        swap(e_sum, e_other, NCH, ch).wait_send()


def exchange(*operands):
    f32, bf16 = jnp.float32, jnp.bfloat16
    dma = pltpu.SemaphoreType.DMA
    hbm = pl.BlockSpec(memory_space=pltpu.HBM)
    vmem = pl.BlockSpec(memory_space=pltpu.VMEM)
    return pl.pallas_call(
        exchange_kernel,
        out_shape=[jax.ShapeDtypeStruct((32, 4096), bf16)] * 2,
        in_specs=[hbm] * 6 + [vmem] * 9,
        out_specs=[vmem] * 2,
        scratch_shapes=[
            pltpu.VMEM((4, 8, 48, 1024), bf16),
            pltpu.VMEM((4096, 512), bf16),
            pltpu.VMEM((256, 4096), bf16),
            pltpu.VMEM((2, 128, 2048), bf16),
            pltpu.VMEM((2, 512, 2048), bf16),
            pltpu.VMEM((256, 128), bf16),
            pltpu.VMEM((2, 256, 512), bf16),
            pltpu.VMEM((15, 8, 128), f32),
            pltpu.VMEM((384, 512), f32),
            pltpu.VMEM((384, 256), bf16),
            pltpu.VMEM((NCH, 2, 8, 48, CW), bf16),
            pltpu.VMEM((NCH, 16, 48, CW), bf16),
        ]
        + [
            pltpu.VMEM((NCH, 4, 64, CW), f32),
            pltpu.VMEM((NCH, 3, 64, CW), f32),
            pltpu.VMEM((NCH, 2, 32, CW), f32),
            pltpu.VMEM((NCH, 32, CW), f32),
        ]
        * 2
        + [
            dma((8, 2)), dma((8, 2)), dma((8, 2)), dma((8, 2)), dma((15,)), dma((15,)),
            dma((7,)), dma((7,)), dma((5,)), dma((NCH, 8, 2)), dma((NCH, 16)),
            dma((NCH, 3)), dma((NCH, 3)), dma((NCH, 3)), dma((NCH, 3)),
            dma((2 * NCH,)), dma((2 * NCH,)),
        ],
        compiler_params=pltpu.CompilerParams(
            collective_id=0, has_side_effects=True, vmem_limit_bytes=60 * 1024 * 1024
        ),
    )(*operands)


def body(
    mixer_rows,
    mixer_gain,
    gate_proj,
    input_proj,
    conv_taps,
    input_gates,
    decay_gates,
    decay_offset,
    out_proj,
    mixer_scale,
    expert_rows,
    expert_gain,
    route_ids,
    route_weights,
    expert_gate,
    expert_up,
    expert_down,
    shared_gate,
    shared_up,
    shared_down,
    expert_scale,
):
    row_count = mixer_rows.shape[0]
    normed = rms_scale(mixer_rows, mixer_gain).astype(jnp.bfloat16)
    gate_branch = jax.nn.gelu(jnp.dot(normed, gate_proj, preferred_element_type=jnp.float32))
    branch = jnp.dot(normed, input_proj, preferred_element_type=jnp.float32).astype(jnp.bfloat16)
    tap_count = conv_taps.shape[0]
    earlier_rows = shifted(branch[row_count - tap_count + 1 :], "ep", 1)
    padded = jnp.concatenate([earlier_rows, branch], axis=0)
    conv_sum = conv_taps[0] * padded[0:row_count].astype(jnp.float32)
    for tap_index in range(1, tap_count):
        conv_sum = conv_sum + conv_taps[tap_index] * padded[
            tap_index : tap_index + row_count
        ].astype(jnp.float32)
    conv_out = conv_sum.astype(jnp.bfloat16)
    block_rows = conv_out.reshape(row_count, input_gates.shape[0], input_gates.shape[1])
    input_gate = jax.nn.sigmoid(
        jnp.einsum("rbi,bij->rbj", block_rows, input_gates, preferred_element_type=jnp.float32)
    ).reshape(row_count, -1)
    decay_gate = jax.nn.sigmoid(
        jnp.einsum("rbi,bij->rbj", block_rows, decay_gates, preferred_element_type=jnp.float32)
    ).reshape(row_count, -1)
    log_decay = -lru_power * decay_gate * jax.nn.softplus(-decay_offset)
    positions = lax.axis_index("ep") * row_count + jnp.arange(row_count, dtype=jnp.int32)
    input_scale = jnp.where((positions == 0)[:, None], 1.0, jnp.sqrt(-jnp.expm1(2.0 * log_decay)))
    drive_term = input_scale * input_gate * conv_out.astype(jnp.float32)
    decay_rate = jnp.exp(log_decay)
    decay_product, local_states = lax.associative_scan(
        linear_pair, (decay_rate, drive_term), axis=0
    )
    carry_message = jnp.concatenate(
        [decay_product[-1].reshape(4, 128), local_states[-1].reshape(4, 128)], axis=0
    )
    tp_index = lax.axis_index("tp")
    y, c = (tp_index // 2, tp_index % 2)
    expert_normed = rms_scale(expert_rows, expert_gain).astype(jnp.bfloat16)
    capacity = 48
    slots = slots_of(route_ids, 16, capacity)
    every = jnp.arange(16 * capacity, dtype=jnp.int32)[None, :]
    mixing = jnp.where(slots[0] == every, route_weights[:, 0:1], 0.0) + jnp.where(
        slots[1] == every, route_weights[:, 1:2], 0.0
    )
    coarse = lax.reduce_precision(mixing, 8, 7)
    mix_high = coarse.astype(jnp.bfloat16)
    mix_low = (mixing - coarse).astype(jnp.bfloat16)
    line = jnp.arange(8 * capacity, dtype=jnp.int32)[None, :]
    owned = (2 * (line // capacity) + c) * capacity + line % capacity
    chosen = jnp.logical_or(slots[0] == owned, slots[1] == owned).astype(jnp.bfloat16)
    outgoing = jnp.stack(
        [
            lax.dot_general(
                chosen,
                lax.dynamic_slice_in_dim(expert_normed, ((y + 2 * j) % 4) * 1024, 1024, axis=1),
                (((0,), (0,)), ((), ())),
                preferred_element_type=jnp.float32,
            )
            .astype(jnp.bfloat16)
            .reshape(8, capacity, 1024)
            for j in range(2)
        ],
        axis=1,
    )
    shared_hidden = (
        jax.nn.silu(jnp.dot(expert_normed, shared_gate, preferred_element_type=jnp.float32))
        * jnp.dot(expert_normed, shared_up, preferred_element_type=jnp.float32)
    ).astype(jnp.bfloat16)
    return tuple(
        exchange(
            outgoing,
            expert_gate[0],
            expert_up[0],
            expert_down[0],
            shared_down,
            out_proj,
            shared_hidden,
            decay_product,
            local_states,
            gate_branch,
            carry_message,
            mix_high,
            mix_low,
            mixer_scale[None, :],
            expert_scale[None, :],
        )
    )


def solution(mesh):
    placed = (
        P("ep", None),
        P(),
        P(None, "tp"),
        P(None, "tp"),
        P(None, "tp"),
        P("tp", None, None),
        P("tp", None, None),
        P("tp"),
        P("tp", None),
        P(),
        P("ep", None),
        P(),
        P("ep", None),
        P("ep", None),
        P("ep", None, "tp"),
        P("ep", None, "tp"),
        P("ep", "tp", None),
        P(None, "tp"),
        P(None, "tp"),
        P("tp", None),
        P(),
    )
    return jax.shard_map(
        body,
        mesh=mesh,
        in_specs=placed,
        out_specs=(P(("ep", "tp"), None), P(("ep", "tp"), None)),
        check_vma=False,
    )
```

```python
import jax
import jax.numpy as jnp
from jax import lax
from jax.experimental import pallas as pl
from jax.experimental.pallas import tpu as pltpu
from jax.sharding import PartitionSpec as P

eps = 1e-06
lru_power = 8.0


MESH = pl.DeviceIdType.MESH
NCH = 4
CW = 2048 // NCH
FAR_EVEN = ((2, 2), (1, 2), (3, 2), (2, 0), (0, 2), (1, 0), (3, 0), (0, 0))
FAR_ODD = ((2, 1), (2, 3), (1, 1), (3, 3), (1, 3), (3, 1), (0, 1), (0, 3))


def remote(src, dst, send, recv, device):
    return pltpu.make_async_remote_copy(
        src_ref=src, dst_ref=dst, send_sem=send, recv_sem=recv, device_id=device, device_id_type=MESH
    )


def hop(step, even, core):
    dz = jnp.where(even, FAR_EVEN[step][0], FAR_ODD[step][0])
    dx = jnp.where(even, FAR_EVEN[step][1], FAR_ODD[step][1])
    return jnp.where(core == 0, dz, (4 - dz) % 4), jnp.where(core == 0, dx, (4 - dx) % 4)


def log1p_small(u):
    series = u * (1 - u * (1 / 2 - u * (1 / 3 - u * (1 / 4 - u * (1 / 5 - u * (1 / 6))))))
    return jnp.where(u < 0.05, series, jnp.log(1.0 + u))


def one_minus_exp(z):
    series = 1.0 + z * (1 / 7)
    for n in (6, 5, 4, 3, 2):
        series = 1.0 + z * series * (1 / n)
    return jnp.where(z > -0.5, -z * series, 1.0 - jnp.exp(z))


def sigmoid(v):
    return 1.0 / (1.0 + jnp.exp(-v))


def whole_kernel(
    m_rows, g_proj, i_proj, i_gates, d_gates, op, x_rows, eg, eu, ed, sg, su, sd,
    m_gain, taps, offset, mscale, x_gain, ids, weights, escale,
    out_m, out_e,
    nx, nm, proj, bgates, send_x, w_sh, br, halo, gate, acum, loc, cm, sh, mix_hi, mix_lo,
    rows, w_in, w_dn, s_dn, o_pr, sh2, gts, carries, acc, hid, res, back,
    m_part, m_recv, m_sum, m_other, e_part, e_recv, e_sum, e_other,
    d_s, d_r, f_s, f_r, c_s, c_r, p_s, p_r, l_s, r_s, r_r, ms_s, ms_r, es_s, es_r, x_s, x_r, h_s, h_r,
):
    f32, bf16 = jnp.float32, jnp.bfloat16
    p = lax.axis_index("ep")
    t = lax.axis_index("tp")
    y = t // 2
    c = t % 2
    o = 1 - c
    z = p // 4
    x = p % 4
    par = p % 2
    half = p // 2
    partner = (p, 2 * y + o)

    def dot(a, b):
        return jnp.dot(a, b, preferred_element_type=f32)

    barrier = pltpu.get_barrier_semaphore()

    def greet(k, _):
        other = (p * 2 + c + k) % 32
        pl.semaphore_signal(
            barrier, inc=1, device_id=(other // 2, 2 * y + other % 2), device_id_type=MESH
        )
        return 0

    lax.fori_loop(1, 32, greet, 0)
    for k in range(1, 4):
        pl.semaphore_signal(
            barrier, inc=1, device_id=(p, 2 * ((y + k) % 4) + c), device_id_type=MESH
        )

    def wide(at):
        return pl.ds(pl.multiple_of(at * 2048, 2048), 2048)

    def local(src, dst, n):
        return pltpu.make_async_copy(src, dst, l_s.at[n])

    first = [local(x_rows.at[:, 1024 * q : 1024 * q + 1024], nx.at[q], q) for q in range(4)]
    second = [local(m_rows, nm, 4), local(i_proj, proj.at[1], 5), local(g_proj, proj.at[0], 6)]
    gates_in = [local(i_gates, bgates.at[0], 7), local(d_gates, bgates.at[1], 8)]
    own_w = [
        local(eg, w_in.at[:, 0:128], 9),
        local(eu, w_in.at[:, 128:256], 10),
        local(ed, w_dn.at[0:128], 11),
    ]
    own_o = local(op.at[:, wide(c)], o_pr.at[0], 12)
    own_s = [
        local(sd.at[:, wide(c)], s_dn.at[0], 13),
        local(sg, w_sh.at[:, 0:128], 14),
        local(su, w_sh.at[:, 128:256], 15),
    ]
    for copy in first:
        copy.start()

    id0, id1 = ids[0:1, :], ids[1:2, :]
    expert = lax.broadcasted_iota(jnp.int32, (16, 256), 0)
    named0, named1 = id0 == expert, id1 == expert
    either = jnp.where(jnp.logical_or(named0, named1), 1.0, 0.0).astype(bf16)
    ahead = jnp.where(
        lax.broadcasted_iota(jnp.int32, (256, 256), 0) < lax.broadcasted_iota(jnp.int32, (256, 256), 1),
        1.0,
        0.0,
    ).astype(bf16)
    place = dot(either, ahead)
    slot0 = id0.astype(f32) * 48.0 + jnp.sum(jnp.where(named0, place, 0.0), axis=0, keepdims=True)
    slot1 = id1.astype(f32) * 48.0 + jnp.sum(jnp.where(named1, place, 0.0), axis=0, keepdims=True)

    def picked(i):
        line = ((2 * i + c) * 48 + lax.broadcasted_iota(jnp.int32, (48, 256), 0)).astype(f32)
        return jnp.where(jnp.logical_or(slot0 == line, slot1 == line), 1.0, 0.0).astype(bf16)

    chosen = jnp.concatenate([picked(i) for i in range(8)], axis=0)

    for copy in first:
        copy.wait()
    for copy in second + gates_in:
        copy.start()

    def norm_x(r, _):
        at = pl.ds(pl.multiple_of(r * 32, 32), 32)
        parts = [nx[q, at, :].astype(f32) for q in range(4)]
        square = sum(jnp.sum(v * v, axis=1, keepdims=True) for v in parts)
        factor = lax.rsqrt(square / 4096.0 + eps)
        for q in range(4):
            nx[q, at, :] = (parts[q] * factor * x_gain[:, 1024 * q : 1024 * q + 1024]).astype(bf16)
        return 0

    lax.fori_loop(0, 8, norm_x, 0)
    for j in range(2):
        send_x[j] = dot(chosen, nx[(y + 2 * j) % 4]).astype(bf16).reshape(8, 48, 1024)

    pl.semaphore_wait(barrier, 34)

    def dispatch(step, j):
        dz, dx = hop(step, par == c, c)
        e = ((z + dz) % 4) * 4 + (x + dx) % 4
        return remote(
            send_x.at[j, e // 2], rows.at[(y + 2 * j) % 4, half], d_s.at[step, j],
            d_r.at[half, j], (e, 2 * y + 1 - par),
        )

    def arrival(step, j):
        dz, dx = hop(step, par == o, par)
        i = (((z + 4 - dz) % 4) * 4 + (x + 4 - dx) % 4) // 2
        return i, remote(send_x.at[j, i], rows.at[(y + 2 * j) % 4, i], d_s.at[step, j], d_r.at[i, j], partner)

    for j in range(2):
        for step in range(8):
            dispatch(step, j).start()

    swaps = [
        remote(sh, sh2, p_s.at[0], p_r.at[0], partner),
        remote(op.at[:, wide(o)], o_pr.at[1], p_s.at[1], p_r.at[1], partner),
        remote(eg, w_in.at[:, 256:384], p_s.at[2], p_r.at[2], partner),
        remote(eu, w_in.at[:, 384:512], p_s.at[3], p_r.at[3], partner),
        remote(ed, w_dn.at[128:256], p_s.at[4], p_r.at[4], partner),
        remote(sd.at[:, wide(o)], s_dn.at[1], p_s.at[5], p_r.at[5], partner),
        remote(gts.at[0], gts.at[1], p_s.at[6], p_r.at[6], partner),
    ]
    for copy in swaps[2:5] + own_w + [swaps[1], own_o, swaps[5]] + own_s:
        copy.start()

    def forward(i, d):
        return remote(
            rows.at[y, i], rows.at[y, i], f_s.at[i, d], f_r.at[i, d],
            (p, 2 * ((y + 1 + 2 * d) % 4) + c),
        )

    def relay(step):
        i, copy = arrival(step, 0)
        copy.wait_recv()
        forward(i, 0).start()
        forward(i, 1).start()

    second[0].wait()

    def norm_m(r, _):
        at = pl.ds(pl.multiple_of(r * 32, 32), 32)
        v = nm[at, :].astype(f32)
        factor = lax.rsqrt(jnp.sum(v * v, axis=1, keepdims=True) / 4096.0 + eps)
        nm[at, :] = (v * factor * m_gain[...]).astype(bf16)
        return 0

    lax.fori_loop(0, 8, norm_m, 0)
    second[1].wait()

    def project(n, _):
        cols = pl.ds(pl.multiple_of(n * 256, 256), 256)
        br[:, cols] = dot(nm[...], proj[1, :, cols]).astype(bf16)
        return 0

    lax.fori_loop(0, 2, project, 0)
    give_halo = remote(br.at[240:256], halo, h_s.at[0], h_r.at[0], ((p + 1) % 16, t))
    give_halo.start()
    relay(0)
    relay(1)
    second[2].wait()

    def gates(n, _):
        cols = pl.ds(pl.multiple_of(n * 256, 256), 256)
        v = dot(nm[...], proj[0, :, cols])
        gate[:, cols] = 0.5 * v * (1.0 + jnp.tanh(0.7978845608028654 * (v + 0.044715 * (v * v * v))))
        return 0

    lax.fori_loop(0, 2, gates, 0)
    relay(2)
    relay(3)
    for copy in gates_in:
        copy.wait()
    give_halo.wait_recv()

    row = lax.broadcasted_iota(jnp.int32, (256, 128), 0)

    def recur(b, _):
        cols = pl.ds(pl.multiple_of(b * 256, 256), 256)
        before = jnp.where(p == 0, 0.0, halo[:, cols].astype(f32))
        ext = jnp.concatenate([before, br[:, cols].astype(f32)], axis=0)
        tap = taps[:, cols]
        conv = tap[0:1] * pltpu.roll(ext, 3, 0)[16:]
        for k in range(1, 4):
            conv = conv + tap[k : k + 1] * (pltpu.roll(ext, 3 - k, 0) if k < 3 else ext)[16:]
        conv_out = conv.astype(bf16)
        gi = sigmoid(dot(conv_out, bgates[0, b]))
        gd = sigmoid(dot(conv_out, bgates[1, b]))
        off = offset[:, cols]
        soft = jnp.maximum(-off, 0.0) + log1p_small(jnp.exp(-jnp.abs(off)))
        log_decay = -lru_power * gd * soft
        scale = jnp.sqrt(one_minus_exp(2.0 * log_decay))
        first_row = jnp.logical_and(lax.broadcasted_iota(jnp.int32, (256, 256), 0) == 0, p == 0)
        scale = jnp.where(first_row, 1.0, scale)
        loc[:, cols] = scale * gi * conv_out.astype(f32)
        acum[:, cols] = jnp.exp(log_decay)
        return 0

    lax.fori_loop(0, 2, recur, 0)
    relay(4)
    relay(5)

    def scan(b, _):
        cols = pl.ds(pl.multiple_of(b * 128, 128), 128)
        av, bv = acum[:, cols], loc[:, cols]
        for d in (1, 2, 4, 8, 16, 32, 64, 128):
            if d < 8:
                a_up = jnp.where(row < d, 1.0, pltpu.roll(av, d, 0))
                b_up = jnp.where(row < d, 0.0, pltpu.roll(bv, d, 0))
            else:
                a_up = jnp.concatenate([jnp.ones((d, 128), f32), av[: 256 - d]], axis=0)
                b_up = jnp.concatenate([jnp.zeros((d, 128), f32), bv[: 256 - d]], axis=0)
            bv = av * b_up + bv
            av = av * a_up
        acum[:, cols] = av
        loc[:, cols] = bv
        cm[pl.ds(b, 1), :] = av[255:256]
        cm[pl.ds(4 + b, 1), :] = bv[255:256]
        return 0

    lax.fori_loop(0, 4, scan, 0)

    def carry(k):
        return remote(cm, carries.at[k - 1], c_s.at[k - 1], c_r.at[k - 1], ((p + k) % 16, t))

    relay(6)
    relay(7)

    def carry_go(k, _):
        carry(k).start()
        return 0

    lax.fori_loop(1, 16, carry_go, 0)

    line = lax.broadcasted_iota(jnp.int32, (128, 256), 0)
    tile = jnp.where(
        line == 0, slot0,
        jnp.where(line == 1, slot1, jnp.where(line == 2, weights[0:1, :], jnp.where(line == 3, weights[1:2, :], 0.0))),
    )
    turned = tile.T
    every = lax.broadcasted_iota(jnp.int32, (256, 768), 1).astype(f32)
    mixing = jnp.where(turned[:, 0:1] == every, turned[:, 2:3], 0.0) + jnp.where(
        turned[:, 1:2] == every, turned[:, 3:4], 0.0
    )
    high = mixing.astype(bf16)
    mix_hi[...] = high
    mix_lo[...] = (mixing - high.astype(f32)).astype(bf16)

    for copy in own_w:
        copy.wait()
    for copy in swaps[2:5]:
        copy.wait_recv()
    for step in range(8):
        i, copy = arrival(step, 1)
        copy.wait_recv()
        for d in range(2):
            source = (y + 3 + 2 * d) % 4
            remote(
                rows.at[source, i], rows.at[source, i], f_s.at[i, d], f_r.at[i, d], partner
            ).wait_recv()

    acc[...] = jnp.zeros_like(acc)

    def quarter(q, _):
        depth = pl.ds(pl.multiple_of(q * 1024, 1024), 1024)
        acc[...] += dot(rows[q].reshape(384, 1024), w_in[depth, :])
        return 0

    lax.fori_loop(0, 4, quarter, 0)
    for side in range(2):
        g = acc[:, 256 * side : 256 * side + 128]
        u = acc[:, 256 * side + 128 : 256 * side + 256]
        hid[:, 128 * side : 128 * side + 128] = (g / (1.0 + jnp.exp(-g)) * u).astype(bf16)

    def returning(ch, step, h):
        dz, dx = hop(step, par == o, c)
        s = ((z + dz) % 4) * 4 + (x + dx) % 4
        return s // 2, s, remote(
            res.at[ch, h, s // 2], back.at[ch, p], r_s.at[ch, step, h], r_r.at[ch, p], (s, 2 * y + h)
        )

    def give(ch, _):
        for h in range(2):
            cols = pl.ds(pl.multiple_of(h * 2048 + ch * CW, CW), CW)
            res[ch, h] = dot(hid[...], w_dn[:, cols]).astype(bf16).reshape(8, 48, CW)
        for h in range(2):
            for step in range(8):
                i, s, copy = returning(ch, step, h)
                if step < 7:
                    copy.start()
                else:

                    @pl.when(jnp.logical_or(s != p, c != h))
                    def _():
                        copy.start()

                    @pl.when(jnp.logical_and(s == p, c == h))
                    def _():
                        back[ch, p] = res[ch, h, i]

        return 0

    lax.fori_loop(0, NCH, give, 0)

    def carry_in(k, _):
        carry(k).wait_recv()
        return 0

    lax.fori_loop(1, 16, carry_in, 0)

    def fold(n, state):
        k = 15 - n
        later = carries[k - 1]
        return jnp.where(k <= p, later[0:4] * state + later[4:8], state)

    state = lax.fori_loop(0, 15, fold, jnp.zeros((4, 128), f32))
    for j in range(4):
        cols = slice(128 * j, 128 * j + 128)
        states = loc[:, cols] + acum[:, cols] * state[j : j + 1]
        gts[0, :, cols] = (gate[:, cols] * states).astype(bf16)

    for copy in own_s:
        copy.wait()
    shared = dot(nx[0], w_sh[0:1024, :])
    for q in range(1, 4):
        shared = shared + dot(nx[q], w_sh[1024 * q : 1024 * q + 1024, :])
    g, u = shared[:, 0:128], shared[:, 128:256]
    swaps[6].start()
    sh[...] = (g / (1.0 + jnp.exp(-g)) * u).astype(bf16)
    own_o.wait()
    swaps[1].wait_recv()
    swaps[6].wait_recv()
    swaps[0].start()

    def scatter(part, recv, send_sem, recv_sem, ch):
        return [
            remote(
                part.at[ch, (y + k) % 4], recv.at[ch, k - 1], send_sem.at[ch, k - 1],
                recv_sem.at[ch, k - 1], (p, 2 * ((y + k) % 4) + c),
            )
            for k in range(1, 4)
        ]

    def swap(total, other, base, ch):
        return remote(
            total.at[ch, o], other.at[ch], x_s.at[base + ch], x_r.at[base + ch], partner
        )

    def settle(part, recv, total, other, send_sem, recv_sem, base):
        def one(ch, _):
            for copy in scatter(part, recv, send_sem, recv_sem, ch):
                copy.wait_recv()
            value = part[ch, y] + recv[ch, 0] + recv[ch, 1] + recv[ch, 2]
            total[ch] = value.reshape(2, 32, CW)
            swap(total, other, base, ch).start()
            return 0

        lax.fori_loop(0, NCH, one, 0)

    def finish(total, other, scale, out, base):
        square = jnp.zeros((32, 1), f32)
        for ch in range(NCH):
            swap(total, other, base, ch).wait_recv()
            mine, theirs = total[ch, c], other[ch]
            square += jnp.sum(mine * mine + theirs * theirs, axis=1, keepdims=True)
        factor = lax.rsqrt(square / 4096.0 + eps)
        for ch in range(NCH):
            for values, side in ((total[ch, c], c), (other[ch], o)):
                cols = pl.ds(pl.multiple_of(side * 2048 + ch * CW, CW), CW)
                out[:, cols] = (values * factor * scale[:, cols]).astype(bf16)

    def mixed(ch, _):
        cols = pl.ds(pl.multiple_of(ch * CW, CW), CW)
        m_part[ch] = (dot(gts[0], o_pr[0, :, cols]) + dot(gts[1], o_pr[1, :, cols])).reshape(4, 64, CW)
        for copy in scatter(m_part, m_recv, ms_s, ms_r, ch):
            copy.start()
        return 0

    lax.fori_loop(0, NCH, mixed, 0)

    swaps[0].wait_recv()
    swaps[5].wait_recv()

    def shared_part(ch, _):
        cols = pl.ds(pl.multiple_of(ch * CW, CW), CW)
        e_part[ch] = (dot(sh[...], s_dn[0, :, cols]) + dot(sh2[...], s_dn[1, :, cols])).reshape(4, 64, CW)
        return 0

    lax.fori_loop(0, NCH, shared_part, 0)

    def combine(ch, _):
        def got(e, _):
            @pl.when(jnp.logical_or(e != p, c != 1 - par))
            def _():
                remote(
                    res.at[ch, 0, 0], back.at[ch, e], r_s.at[ch, 0, 0], r_r.at[ch, e], partner
                ).wait_recv()

            return 0

        lax.fori_loop(0, 16, got, 0)
        returned = back[ch].reshape(768, CW)
        e_part[ch] = e_part[ch] + (
            dot(mix_hi[...], returned) + dot(mix_lo[...], returned)
        ).reshape(4, 64, CW)
        for copy in scatter(e_part, e_recv, es_s, es_r, ch):
            copy.start()
        return 0

    lax.fori_loop(0, NCH - 1, combine, 0)
    settle(m_part, m_recv, m_sum, m_other, ms_s, ms_r, 0)
    finish(m_sum, m_other, mscale, out_m, 0)
    combine(NCH - 1, 0)
    settle(e_part, e_recv, e_sum, e_other, es_s, es_r, NCH)
    finish(e_sum, e_other, escale, out_e, NCH)

    for step in range(8):
        for j in range(2):
            dispatch(step, j).wait_send()
            forward(step, j).wait_send()

    def drain(ch, _):
        for step in range(8):
            for h in range(2):
                i, s, copy = returning(ch, step, h)
                if step < 7:
                    copy.wait_send()
                else:

                    @pl.when(jnp.logical_or(s != p, c != h))
                    def _():
                        copy.wait_send()

        for copy in scatter(m_part, m_recv, ms_s, ms_r, ch):
            copy.wait_send()
        for copy in scatter(e_part, e_recv, es_s, es_r, ch):
            copy.wait_send()
        swap(m_sum, m_other, 0, ch).wait_send()
        swap(e_sum, e_other, NCH, ch).wait_send()
        return 0

    lax.fori_loop(0, NCH, drain, 0)

    def carry_out(k, _):
        carry(k).wait_send()
        return 0

    lax.fori_loop(1, 16, carry_out, 0)
    for copy in swaps:
        copy.wait_send()
    give_halo.wait_send()


def body(
    mixer_rows, mixer_gain, gate_proj, input_proj, conv_taps, input_gates, decay_gates,
    decay_offset, out_proj, mixer_scale, expert_rows, expert_gain, route_ids, route_weights,
    expert_gate, expert_up, expert_down, shared_gate, shared_up, shared_down, expert_scale,
):
    f32, bf16 = jnp.float32, jnp.bfloat16
    dma = pltpu.SemaphoreType.DMA
    hbm = pl.BlockSpec(memory_space=pltpu.HBM)
    vmem = pl.BlockSpec(memory_space=pltpu.VMEM)
    outs = pl.pallas_call(
        whole_kernel,
        out_shape=[jax.ShapeDtypeStruct((32, 4096), bf16)] * 2,
        in_specs=[hbm] * 13 + [vmem] * 8,
        out_specs=[vmem] * 2,
        scratch_shapes=[
            pltpu.VMEM((4, 256, 1024), bf16),
            pltpu.VMEM((256, 4096), bf16),
            pltpu.VMEM((2, 4096, 512), bf16),
            pltpu.VMEM((2, 2, 256, 256), bf16),
            pltpu.VMEM((2, 8, 48, 1024), bf16),
            pltpu.VMEM((4096, 256), bf16),
            pltpu.VMEM((256, 512), bf16),
            pltpu.VMEM((16, 512), bf16),
            pltpu.VMEM((256, 512), f32),
            pltpu.VMEM((256, 512), f32),
            pltpu.VMEM((256, 512), f32),
            pltpu.VMEM((8, 128), f32),
            pltpu.VMEM((256, 128), bf16),
            pltpu.VMEM((256, 768), bf16),
            pltpu.VMEM((256, 768), bf16),
            pltpu.VMEM((4, 8, 48, 1024), bf16),
            pltpu.VMEM((4096, 512), bf16),
            pltpu.VMEM((256, 4096), bf16),
            pltpu.VMEM((2, 128, 2048), bf16),
            pltpu.VMEM((2, 512, 2048), bf16),
            pltpu.VMEM((256, 128), bf16),
            pltpu.VMEM((2, 256, 512), bf16),
            pltpu.VMEM((15, 8, 128), f32),
            pltpu.VMEM((384, 512), f32),
            pltpu.VMEM((384, 256), bf16),
            pltpu.VMEM((NCH, 2, 8, 48, CW), bf16),
            pltpu.VMEM((NCH, 16, 48, CW), bf16),
        ]
        + [
            pltpu.VMEM((NCH, 4, 64, CW), f32),
            pltpu.VMEM((NCH, 3, 64, CW), f32),
            pltpu.VMEM((NCH, 2, 32, CW), f32),
            pltpu.VMEM((NCH, 32, CW), f32),
        ]
        * 2
        + [
            dma((8, 2)), dma((8, 2)), dma((8, 2)), dma((8, 2)), dma((15,)), dma((15,)),
            dma((7,)), dma((7,)), dma((16,)), dma((NCH, 8, 2)), dma((NCH, 16)),
            dma((NCH, 3)), dma((NCH, 3)), dma((NCH, 3)), dma((NCH, 3)),
            dma((2 * NCH,)), dma((2 * NCH,)), dma((1,)), dma((1,)),
        ],
        compiler_params=pltpu.CompilerParams(
            collective_id=0, has_side_effects=True, vmem_limit_bytes=67043328
        ),
    )(
        mixer_rows, gate_proj, input_proj, input_gates, decay_gates, out_proj, expert_rows,
        expert_gate[0], expert_up[0], expert_down[0], shared_gate, shared_up, shared_down,
        mixer_gain[None, :], conv_taps, decay_offset[None, :], mixer_scale[None, :],
        expert_gain[None, :], route_ids.T, route_weights.T, expert_scale[None, :],
    )
    return tuple(outs)


def solution(mesh):
    placed = (
        P("ep", None),
        P(),
        P(None, "tp"),
        P(None, "tp"),
        P(None, "tp"),
        P("tp", None, None),
        P("tp", None, None),
        P("tp"),
        P("tp", None),
        P(),
        P("ep", None),
        P(),
        P("ep", None),
        P("ep", None),
        P("ep", None, "tp"),
        P("ep", None, "tp"),
        P("ep", "tp", None),
        P(None, "tp"),
        P(None, "tp"),
        P("tp", None),
        P(),
    )
    return jax.shard_map(
        body,
        mesh=mesh,
        in_specs=placed,
        out_specs=(P(("ep", "tp"), None), P(("ep", "tp"), None)),
        check_vma=False,
    )
```

```python
import jax
import jax.numpy as jnp
from jax import lax
from jax.experimental import pallas as pl
from jax.experimental.pallas import tpu as pltpu
from jax.sharding import PartitionSpec as P

eps = 1e-06
lru_power = 8.0


MESH = pl.DeviceIdType.MESH
NCH = 8
FAR = 6
ORDER0 = (5, 4, 3, 2, 1, 0)
CW = 2048 // NCH
FAR_EVEN = ((2, 2), (1, 2), (3, 2), (2, 0), (0, 2), (1, 0), (3, 0), (0, 0))
FAR_ODD = ((2, 1), (2, 3), (1, 1), (3, 3), (1, 3), (3, 1), (0, 1), (0, 3))


def remote(src, dst, send, recv, device):
    return pltpu.make_async_remote_copy(
        src_ref=src, dst_ref=dst, send_sem=send, recv_sem=recv, device_id=device, device_id_type=MESH
    )


def hop(step, even, core):
    dz = jnp.where(even, FAR_EVEN[step][0], FAR_ODD[step][0])
    dx = jnp.where(even, FAR_EVEN[step][1], FAR_ODD[step][1])
    return jnp.where(core == 0, dz, (4 - dz) % 4), jnp.where(core == 0, dx, (4 - dx) % 4)


def log1p_small(u):
    series = u * (1 - u * (1 / 2 - u * (1 / 3 - u * (1 / 4 - u * (1 / 5 - u * (1 / 6))))))
    return jnp.where(u < 0.05, series, jnp.log(1.0 + u))


def one_minus_exp(z):
    series = 1.0 + z * (1 / 7)
    for n in (6, 5, 4, 3, 2):
        series = 1.0 + z * series * (1 / n)
    return jnp.where(z > -0.5, -z * series, 1.0 - jnp.exp(z))


def sigmoid(v):
    return 1.0 / (1.0 + jnp.exp(-v))


def whole_kernel(
    m_rows, g_proj, i_proj, i_gates, d_gates, op, x_rows, eg, eu, ed, sg, su, sd,
    m_gain_h, taps_h, offset_h, mscale_h, x_gain_h, ids_h, weights_h, escale_h,
    out_m, out_e,
    m_gain, taps, offset, mscale, x_gain, ids, weights, escale,
    nx, nm, proj, bgates, send_x, send_n, w_sh, br, tail, edge, halo, gate, acum, loc, cm, sh, mix_hi, mix_lo,
    rows, w_in, w_dn, s_dn, o_pr, sh2, gts, carries, acc, hid, res, back,
    m_part, m_send, m_recv, m_sum, m_other, e_part, e_recv, e_sum, e_other,
    d_s, d_r, f_s, f_r, c_s, c_r, p_s, p_r, l_s, r_s, r_r, ms_s, ms_r, es_s, es_r, x_s, x_r, h_s, h_r,
):
    f32, bf16 = jnp.float32, jnp.bfloat16
    p = lax.axis_index("ep")
    t = lax.axis_index("tp")
    y = t // 2
    c = t % 2
    o = 1 - c
    z = p // 4
    x = p % 4
    par = p % 2
    half = p // 2
    partner = (p, 2 * y + o)

    def dot(a, b):
        return jnp.dot(a, b, preferred_element_type=f32)

    barrier = pltpu.get_barrier_semaphore()

    def greet(k, _):
        other = (p * 2 + c + k) % 32
        pl.semaphore_signal(
            barrier, inc=1, device_id=(other // 2, 2 * y + other % 2), device_id_type=MESH
        )
        return 0

    lax.fori_loop(1, 32, greet, 0)
    for k in range(1, 4):
        pl.semaphore_signal(
            barrier, inc=1, device_id=(p, 2 * ((y + k) % 4) + c), device_id_type=MESH
        )

    def wide(at):
        return pl.ds(pl.multiple_of(at * 2048, 2048), 2048)

    def local(src, dst, n):
        return pltpu.make_async_copy(src, dst, l_s.at[n])

    early = [local(m_rows.at[240:256], tail, 16), local(i_proj, proj.at[1], 5)]
    first = [local(x_rows.at[:, 1024 * q : 1024 * q + 1024], nx.at[q], q) for q in range(4)]
    second = [local(m_rows, nm, 4), local(g_proj, proj.at[0], 6)]
    gates_in = [local(i_gates, bgates.at[0], 7), local(d_gates, bgates.at[1], 8)]
    own_w = [
        local(eg, w_in.at[:, 0:128], 9),
        local(eu, w_in.at[:, 128:256], 10),
        local(ed, w_dn.at[0:128], 11),
    ]
    own_o = local(op.at[:, wide(c)], o_pr.at[0], 12)
    own_s = [
        local(sd.at[:, wide(c)], s_dn.at[0], 13),
        local(sg, w_sh.at[:, 0:128], 14),
        local(su, w_sh.at[:, 128:256], 15),
    ]
    small = [local(ids_h, ids, 17), local(weights_h, weights, 18), local(x_gain_h, x_gain, 19)]
    small += [local(m_gain_h, m_gain, 20), local(taps_h, taps, 21), local(offset_h, offset, 22)]
    small += [local(mscale_h, mscale, 23), local(escale_h, escale, 24)]
    for copy in small[:1] + first + small[1:]:
        copy.start()
    small[0].wait()

    id0, id1 = ids[0:1, :], ids[1:2, :]
    expert = lax.broadcasted_iota(jnp.int32, (16, 256), 0)
    named0, named1 = id0 == expert, id1 == expert
    either = jnp.where(jnp.logical_or(named0, named1), 1.0, 0.0).astype(bf16)
    ahead = jnp.where(
        lax.broadcasted_iota(jnp.int32, (256, 256), 0) < lax.broadcasted_iota(jnp.int32, (256, 256), 1),
        1.0,
        0.0,
    ).astype(bf16)
    place = dot(either, ahead)
    slot0 = id0.astype(f32) * 48.0 + jnp.sum(jnp.where(named0, place, 0.0), axis=0, keepdims=True)
    slot1 = id1.astype(f32) * 48.0 + jnp.sum(jnp.where(named1, place, 0.0), axis=0, keepdims=True)

    def picked(i):
        line = ((2 * i + c) * 48 + lax.broadcasted_iota(jnp.int32, (48, 256), 0)).astype(f32)
        return jnp.where(jnp.logical_or(slot0 == line, slot1 == line), 1.0, 0.0).astype(bf16)

    chosen = jnp.concatenate([picked(i) for i in range(8)], axis=0)

    for copy in first + small[1:]:
        copy.wait()
    for copy in early + second + gates_in:
        copy.start()

    def norm_x(r, _):
        at = pl.ds(pl.multiple_of(r * 32, 32), 32)
        parts = [nx[q, at, :].astype(f32) for q in range(4)]
        square = sum(jnp.sum(v * v, axis=1, keepdims=True) for v in parts)
        factor = lax.rsqrt(square / 4096.0 + eps)
        for q in range(4):
            nx[q, at, :] = (parts[q] * factor * x_gain[:, 1024 * q : 1024 * q + 1024]).astype(bf16)
        return 0

    lax.fori_loop(0, 8, norm_x, 0)
    for j in range(2):
        send_x[j] = dot(chosen, nx[(y + 2 * j) % 4]).astype(bf16).reshape(8, 48, 1024)
    near = []
    for step in range(FAR, 8):
        dz, dx = hop(step, par == c, c)
        near.append(((((z + dz) % 4) * 4 + (x + dx) % 4) // 2))
    near_chosen = jnp.concatenate([picked(i) for i in near], axis=0)
    for j in range(2):
        send_n[j] = dot(near_chosen, nx[(y + 1 + 2 * j) % 4]).astype(bf16).reshape(8 - FAR, 48, 1024)

    for copy in early:
        copy.wait()
    v = tail[...].astype(f32)
    factor = lax.rsqrt(jnp.sum(v * v, axis=1, keepdims=True) / 4096.0 + eps)
    last_rows = (v * factor * m_gain[...]).astype(bf16)
    edge[...] = dot(last_rows, proj[1]).astype(bf16)

    pl.semaphore_wait(barrier, 34)
    give_halo = remote(edge, halo, h_s.at[0], h_r.at[0], ((p + 1) % 16, t))
    give_halo.start()

    def dispatch(step, j):
        dz, dx = hop(step, par == c, c)
        e = ((z + dz) % 4) * 4 + (x + dx) % 4
        source = send_x.at[j, e // 2] if j < 2 else send_n.at[j - 2, step - FAR]
        shift = (0, 2, 1, 3)[j]
        return remote(
            source, rows.at[(y + shift) % 4, step], d_s.at[step, j], d_r.at[step, j],
            (e, 2 * y + 1 - par),
        )

    def arrival(step, j):
        shift = (0, 2, 1, 3)[j]
        return remote(
            send_x.at[0, 0], rows.at[(y + shift) % 4, step], d_s.at[step, j], d_r.at[step, j], partner
        )

    order = [(step, 0) for step in ORDER0] + [(step, 1) for step in range(8)]
    order += [(step, j) for step in range(FAR, 8) for j in (0, 2, 3)]
    for step, j in order:
        dispatch(step, j).start()

    swaps = [
        remote(sh, sh2, p_s.at[0], p_r.at[0], partner),
        remote(op.at[:, wide(o)], o_pr.at[1], p_s.at[1], p_r.at[1], partner),
        remote(eg, w_in.at[:, 256:384], p_s.at[2], p_r.at[2], partner),
        remote(eu, w_in.at[:, 384:512], p_s.at[3], p_r.at[3], partner),
        remote(ed, w_dn.at[128:256], p_s.at[4], p_r.at[4], partner),
        remote(sd.at[:, wide(o)], s_dn.at[1], p_s.at[5], p_r.at[5], partner),
        remote(gts.at[0], gts.at[1], p_s.at[6], p_r.at[6], partner),
    ]
    for copy in swaps[2:5] + own_w + [swaps[1], own_o, swaps[5]] + own_s:
        copy.start()

    def forward(i, d):
        return remote(
            rows.at[y, i], rows.at[y, i], f_s.at[i, d], f_r.at[i, d],
            (p, 2 * ((y + 1 + 2 * d) % 4) + c),
        )

    def relay(step):
        arrival(step, 0).wait_recv()
        forward(step, 0).start()
        forward(step, 1).start()

    second[0].wait()

    def norm_m(r, _):
        at = pl.ds(pl.multiple_of(r * 32, 32), 32)
        v = nm[at, :].astype(f32)
        factor = lax.rsqrt(jnp.sum(v * v, axis=1, keepdims=True) / 4096.0 + eps)
        nm[at, :] = (v * factor * m_gain[...]).astype(bf16)
        return 0

    lax.fori_loop(0, 8, norm_m, 0)

    def project(n, _):
        cols = pl.ds(pl.multiple_of(n * 256, 256), 256)
        br[:, cols] = dot(nm[...], proj[1, :, cols]).astype(bf16)
        return 0

    lax.fori_loop(0, 2, project, 0)
    second[1].wait()

    def gates(n, _):
        cols = pl.ds(pl.multiple_of(n * 256, 256), 256)
        v = dot(nm[...], proj[0, :, cols])
        gate[:, cols] = 0.5 * v * (1.0 + jnp.tanh(0.7978845608028654 * (v + 0.044715 * (v * v * v))))
        return 0

    lax.fori_loop(0, 2, gates, 0)
    for copy in gates_in:
        copy.wait()
    give_halo.wait_recv()

    row = lax.broadcasted_iota(jnp.int32, (256, 128), 0)

    def recur(b, _):
        cols = pl.ds(pl.multiple_of(b * 256, 256), 256)
        before = jnp.where(p == 0, 0.0, halo[:, cols].astype(f32))
        ext = jnp.concatenate([before, br[:, cols].astype(f32)], axis=0)
        tap = taps[:, cols]
        conv = tap[0:1] * pltpu.roll(ext, 3, 0)[16:]
        for k in range(1, 4):
            conv = conv + tap[k : k + 1] * (pltpu.roll(ext, 3 - k, 0) if k < 3 else ext)[16:]
        conv_out = conv.astype(bf16)
        gi = sigmoid(dot(conv_out, bgates[0, b]))
        gd = sigmoid(dot(conv_out, bgates[1, b]))
        off = offset[:, cols]
        soft = jnp.maximum(-off, 0.0) + log1p_small(jnp.exp(-jnp.abs(off)))
        log_decay = -lru_power * gd * soft
        scale = jnp.sqrt(one_minus_exp(2.0 * log_decay))
        first_row = jnp.logical_and(lax.broadcasted_iota(jnp.int32, (256, 256), 0) == 0, p == 0)
        scale = jnp.where(first_row, 1.0, scale)
        loc[:, cols] = scale * gi * conv_out.astype(f32)
        acum[:, cols] = jnp.exp(log_decay)
        return 0

    for step in ORDER0[:2]:
        relay(step)
    recur(0, 0)
    for step in ORDER0[2:4]:
        relay(step)
    recur(1, 0)
    for step in ORDER0[4:]:
        relay(step)

    def scan(b, _):
        cols = pl.ds(pl.multiple_of(b * 128, 128), 128)
        av, bv = acum[:, cols], loc[:, cols]
        for d in (1, 2, 4, 8, 16, 32, 64, 128):
            if d < 8:
                a_up = jnp.where(row < d, 1.0, pltpu.roll(av, d, 0))
                b_up = jnp.where(row < d, 0.0, pltpu.roll(bv, d, 0))
            else:
                a_up = jnp.concatenate([jnp.ones((d, 128), f32), av[: 256 - d]], axis=0)
                b_up = jnp.concatenate([jnp.zeros((d, 128), f32), bv[: 256 - d]], axis=0)
            bv = av * b_up + bv
            av = av * a_up
        acum[:, cols] = av
        loc[:, cols] = bv
        cm[pl.ds(b, 1), :] = av[255:256]
        cm[pl.ds(4 + b, 1), :] = bv[255:256]
        return 0

    lax.fori_loop(0, 4, scan, 0)

    def carry(k):
        return remote(cm, carries.at[k - 1], c_s.at[k - 1], c_r.at[k - 1], ((p + k) % 16, t))

    def carry_go(k, _):
        carry(k).start()
        return 0

    lax.fori_loop(1, 16, carry_go, 0)
    line = lax.broadcasted_iota(jnp.int32, (128, 256), 0)
    tile = jnp.where(
        line == 0, slot0,
        jnp.where(line == 1, slot1, jnp.where(line == 2, weights[0:1, :], jnp.where(line == 3, weights[1:2, :], 0.0))),
    )
    turned = tile.T
    every = lax.broadcasted_iota(jnp.int32, (256, 768), 1).astype(f32)
    mixing = jnp.where(turned[:, 0:1] == every, turned[:, 2:3], 0.0) + jnp.where(
        turned[:, 1:2] == every, turned[:, 3:4], 0.0
    )
    high = mixing.astype(bf16)
    mix_hi[...] = high
    mix_lo[...] = (mixing - high.astype(f32)).astype(bf16)

    for copy in own_s:
        copy.wait()
    shared = dot(nx[0], w_sh[0:1024, :])
    for q in range(1, 4):
        shared = shared + dot(nx[q], w_sh[1024 * q : 1024 * q + 1024, :])
    g, u = shared[:, 0:128], shared[:, 128:256]
    sh[...] = (g / (1.0 + jnp.exp(-g)) * u).astype(bf16)
    swaps[0].start()

    def scatter(part, recv, send_sem, recv_sem, ch):
        return [
            remote(
                part.at[ch, (y + k) % 4], recv.at[ch, k - 1], send_sem.at[ch, k - 1],
                recv_sem.at[ch, k - 1], (p, 2 * ((y + k) % 4) + c),
            )
            for k in range(1, 4)
        ]

    def swap(total, other, base, ch):
        return remote(
            total.at[ch, o], other.at[ch], x_s.at[base + ch], x_r.at[base + ch], partner
        )

    def settle(part, sent, recv, total, other, send_sem, recv_sem, base):
        def one(ch, _):
            for copy in scatter(sent, recv, send_sem, recv_sem, ch):
                copy.wait_recv()
            value = part[ch, y] + sum(recv[ch, k].astype(f32) for k in range(3))
            total[ch] = value.reshape(2, 32, CW)
            swap(total, other, base, ch).start()
            return 0

        lax.fori_loop(0, NCH, one, 0)

    def finish(total, other, scale, out, base):
        square = jnp.zeros((32, 1), f32)
        for ch in range(NCH):
            swap(total, other, base, ch).wait_recv()
            mine, theirs = total[ch, c], other[ch]
            square += jnp.sum(mine * mine + theirs * theirs, axis=1, keepdims=True)
        factor = lax.rsqrt(square / 4096.0 + eps)
        for ch in range(NCH):
            for values, side in ((total[ch, c], c), (other[ch], o)):
                cols = pl.ds(pl.multiple_of(side * 2048 + ch * CW, CW), CW)
                out[:, cols] = (values * factor * scale[:, cols]).astype(bf16)

    swaps[0].wait_recv()
    swaps[5].wait_recv()

    def shared_part(ch, _):
        cols = pl.ds(pl.multiple_of(ch * CW, CW), CW)
        e_part[ch] = (dot(sh[...], s_dn[0, :, cols]) + dot(sh2[...], s_dn[1, :, cols])).reshape(4, 64, CW)
        return 0

    lax.fori_loop(0, NCH, shared_part, 0)

    for copy in own_w:
        copy.wait()
    for copy in swaps[2:5]:
        copy.wait_recv()

    def quarter(q):
        depth = pl.ds(pl.multiple_of(q * 1024, 1024), 1024)
        return dot(rows[q].reshape(384, 1024), w_in[depth, :])

    for step in range(FAR, 8):
        arrival(step, 0).wait_recv()
    acc[...] = quarter(y)
    for step in range(8):
        arrival(step, 1).wait_recv()
    acc[...] += quarter((y + 2) % 4)
    for d in range(2):
        source = (y + 3 + 2 * d) % 4
        for step in range(FAR, 8):
            arrival(step, 3 - d).wait_recv()
        for step in range(FAR):
            remote(
                rows.at[source, step], rows.at[source, step], f_s.at[step, d], f_r.at[step, d], partner
            ).wait_recv()
        acc[...] += quarter(source)
    for side in range(2):
        g = acc[:, 256 * side : 256 * side + 128]
        u = acc[:, 256 * side + 128 : 256 * side + 256]
        hid[:, 128 * side : 128 * side + 128] = (g / (1.0 + jnp.exp(-g)) * u).astype(bf16)

    def returning(ch, step, h):
        dz, dx = hop(step, par == o, par)
        s = ((z + 4 - dz) % 4) * 4 + (x + 4 - dx) % 4
        return step, s, remote(
            res.at[ch, h, step], back.at[ch, p], r_s.at[ch, step, h], r_r.at[ch, p], (s, 2 * y + h)
        )

    def give(ch, _):
        for h in range(2):
            cols = pl.ds(pl.multiple_of(h * 2048 + ch * CW, CW), CW)
            res[ch, h] = dot(hid[...], w_dn[:, cols]).astype(bf16).reshape(8, 48, CW)
        for h in range(2):
            for step in range(8):
                i, s, copy = returning(ch, step, h)
                if step < 7:
                    copy.start()
                else:

                    @pl.when(jnp.logical_or(s != p, c != h))
                    def _():
                        copy.start()

                    @pl.when(jnp.logical_and(s == p, c == h))
                    def _():
                        back[ch, p] = res[ch, h, i]

        return 0

    lax.fori_loop(0, NCH, give, 0)

    def carry_in(k, _):
        carry(k).wait_recv()
        return 0

    lax.fori_loop(1, 16, carry_in, 0)

    def fold(n, state):
        k = 15 - n
        later = carries[k - 1]
        return jnp.where(k <= p, later[0:4] * state + later[4:8], state)

    state = lax.fori_loop(0, 15, fold, jnp.zeros((4, 128), f32))
    for j in range(4):
        cols = slice(128 * j, 128 * j + 128)
        states = loc[:, cols] + acum[:, cols] * state[j : j + 1]
        gts[0, :, cols] = (gate[:, cols] * states).astype(bf16)

    swaps[6].start()

    own_o.wait()
    swaps[1].wait_recv()
    swaps[6].wait_recv()

    def mixed(ch, _):
        cols = pl.ds(pl.multiple_of(ch * CW, CW), CW)
        m_part[ch] = (dot(gts[0], o_pr[0, :, cols]) + dot(gts[1], o_pr[1, :, cols])).reshape(4, 64, CW)
        m_send[ch] = m_part[ch].astype(bf16)
        for copy in scatter(m_send, m_recv, ms_s, ms_r, ch):
            copy.start()
        return 0

    lax.fori_loop(0, NCH, mixed, 0)

    def combine(ch, _):
        def got(e, _):
            @pl.when(jnp.logical_or(e != p, c != 1 - par))
            def _():
                remote(
                    res.at[ch, 0, 0], back.at[ch, e], r_s.at[ch, 0, 0], r_r.at[ch, e], partner
                ).wait_recv()

            return 0

        lax.fori_loop(0, 16, got, 0)
        returned = back[ch].reshape(768, CW)
        e_part[ch] = e_part[ch] + (
            dot(mix_hi[...], returned) + dot(mix_lo[...], returned)
        ).reshape(4, 64, CW)
        for copy in scatter(e_part, e_recv, es_s, es_r, ch):
            copy.start()
        return 0

    lax.fori_loop(0, NCH // 2, combine, 0)
    settle(m_part, m_send, m_recv, m_sum, m_other, ms_s, ms_r, 0)
    finish(m_sum, m_other, mscale, out_m, 0)
    lax.fori_loop(NCH // 2, NCH, combine, 0)
    for step, j in order:
        dispatch(step, j).wait_send()
    for step in range(FAR):
        for d in range(2):
            forward(step, d).wait_send()

    def drain(ch, _):
        for step in range(8):
            for h in range(2):
                i, s, copy = returning(ch, step, h)
                if step < 7:
                    copy.wait_send()
                else:

                    @pl.when(jnp.logical_or(s != p, c != h))
                    def _():
                        copy.wait_send()

        for copy in scatter(m_send, m_recv, ms_s, ms_r, ch):
            copy.wait_send()
        swap(m_sum, m_other, 0, ch).wait_send()
        return 0

    lax.fori_loop(0, NCH, drain, 0)

    def carry_out(k, _):
        carry(k).wait_send()
        return 0

    lax.fori_loop(1, 16, carry_out, 0)
    for copy in swaps:
        copy.wait_send()
    give_halo.wait_send()

    settle(e_part, e_part, e_recv, e_sum, e_other, es_s, es_r, NCH)
    finish(e_sum, e_other, escale, out_e, NCH)

    def drain_last(ch, _):
        for copy in scatter(e_part, e_recv, es_s, es_r, ch):
            copy.wait_send()
        swap(e_sum, e_other, NCH, ch).wait_send()
        return 0

    lax.fori_loop(0, NCH, drain_last, 0)


def body(
    mixer_rows, mixer_gain, gate_proj, input_proj, conv_taps, input_gates, decay_gates,
    decay_offset, out_proj, mixer_scale, expert_rows, expert_gain, route_ids, route_weights,
    expert_gate, expert_up, expert_down, shared_gate, shared_up, shared_down, expert_scale,
):
    f32, bf16 = jnp.float32, jnp.bfloat16
    dma = pltpu.SemaphoreType.DMA
    hbm = pl.BlockSpec(memory_space=pltpu.HBM)
    vmem = pl.BlockSpec(memory_space=pltpu.VMEM)
    outs = pl.pallas_call(
        whole_kernel,
        out_shape=[jax.ShapeDtypeStruct((32, 4096), bf16)] * 2,
        in_specs=[hbm] * 21,
        out_specs=[vmem] * 2,
        scratch_shapes=[
            pltpu.VMEM((1, 4096), f32),
            pltpu.VMEM((4, 512), f32),
            pltpu.VMEM((1, 512), f32),
            pltpu.VMEM((1, 4096), f32),
            pltpu.VMEM((1, 4096), f32),
            pltpu.VMEM((2, 256), jnp.int32),
            pltpu.VMEM((2, 256), f32),
            pltpu.VMEM((1, 4096), f32),
            pltpu.VMEM((4, 256, 1024), bf16),
            pltpu.VMEM((256, 4096), bf16),
            pltpu.VMEM((2, 4096, 512), bf16),
            pltpu.VMEM((2, 2, 256, 256), bf16),
            pltpu.VMEM((2, 8, 48, 1024), bf16),
            pltpu.VMEM((2, 8 - FAR, 48, 1024), bf16),
            pltpu.VMEM((4096, 256), bf16),
            pltpu.VMEM((256, 512), bf16),
            pltpu.VMEM((16, 4096), bf16),
            pltpu.VMEM((16, 512), bf16),
            pltpu.VMEM((16, 512), bf16),
            pltpu.VMEM((256, 512), f32),
            pltpu.VMEM((256, 512), f32),
            pltpu.VMEM((256, 512), f32),
            pltpu.VMEM((8, 128), f32),
            pltpu.VMEM((256, 128), bf16),
            pltpu.VMEM((256, 768), bf16),
            pltpu.VMEM((256, 768), bf16),
            pltpu.VMEM((4, 8, 48, 1024), bf16),
            pltpu.VMEM((4096, 512), bf16),
            pltpu.VMEM((256, 4096), bf16),
            pltpu.VMEM((2, 128, 2048), bf16),
            pltpu.VMEM((2, 512, 2048), bf16),
            pltpu.VMEM((256, 128), bf16),
            pltpu.VMEM((2, 256, 512), bf16),
            pltpu.VMEM((15, 8, 128), f32),
            pltpu.VMEM((384, 512), f32),
            pltpu.VMEM((384, 256), bf16),
            pltpu.VMEM((NCH, 2, 8, 48, CW), bf16),
            pltpu.VMEM((NCH, 16, 48, CW), bf16),
        ]
        + [
            pltpu.VMEM((NCH, 4, 64, CW), f32),
            pltpu.VMEM((NCH, 4, 64, CW), bf16),
            pltpu.VMEM((NCH, 3, 64, CW), bf16),
            pltpu.VMEM((NCH, 2, 32, CW), f32),
            pltpu.VMEM((NCH, 32, CW), f32),
            pltpu.VMEM((NCH, 4, 64, CW), f32),
            pltpu.VMEM((NCH, 3, 64, CW), f32),
            pltpu.VMEM((NCH, 2, 32, CW), f32),
            pltpu.VMEM((NCH, 32, CW), f32),
        ]
        + [
            dma((8, 4)), dma((8, 4)), dma((8, 2)), dma((8, 2)), dma((15,)), dma((15,)),
            dma((7,)), dma((7,)), dma((25,)), dma((NCH, 8, 2)), dma((NCH, 16)),
            dma((NCH, 3)), dma((NCH, 3)), dma((NCH, 3)), dma((NCH, 3)),
            dma((2 * NCH,)), dma((2 * NCH,)), dma((1,)), dma((1,)),
        ],
        compiler_params=pltpu.CompilerParams(
            collective_id=0, has_side_effects=True, vmem_limit_bytes=67043328
        ),
    )(
        mixer_rows, gate_proj, input_proj, input_gates, decay_gates, out_proj, expert_rows,
        expert_gate[0], expert_up[0], expert_down[0], shared_gate, shared_up, shared_down,
        mixer_gain[None, :], conv_taps, decay_offset[None, :], mixer_scale[None, :],
        expert_gain[None, :], route_ids.T, route_weights.T, expert_scale[None, :],
    )

    def hand_out(a, b, a_out, b_out):
        a_out[...] = a[...]
        b_out[...] = b[...]

    return tuple(
        pl.pallas_call(
            hand_out,
            out_shape=[jax.ShapeDtypeStruct((32, 4096), bf16)] * 2,
            in_specs=[vmem] * 2,
            out_specs=[vmem] * 2,
        )(*outs)
    )


def solution(mesh):
    placed = (
        P("ep", None),
        P(),
        P(None, "tp"),
        P(None, "tp"),
        P(None, "tp"),
        P("tp", None, None),
        P("tp", None, None),
        P("tp"),
        P("tp", None),
        P(),
        P("ep", None),
        P(),
        P("ep", None),
        P("ep", None),
        P("ep", None, "tp"),
        P("ep", None, "tp"),
        P("ep", "tp", None),
        P(None, "tp"),
        P(None, "tp"),
        P("tp", None),
        P(),
    )
    return jax.shard_map(
        body,
        mesh=mesh,
        in_specs=placed,
        out_specs=(P(("ep", "tp"), None), P(("ep", "tp"), None)),
        check_vma=False,
    )
```

```python
import jax
import jax.numpy as jnp
from jax import lax
from jax.experimental import pallas as pl
from jax.experimental.pallas import tpu as pltpu
from jax.sharding import PartitionSpec as P

eps = 1e-06
lru_power = 8.0


MESH = pl.DeviceIdType.MESH
NCH = 8
FAR = 6
LEAD = 2
CW = 2048 // NCH
FAR_EVEN = ((2, 2), (1, 2), (3, 2), (2, 0), (0, 2), (1, 0), (3, 0), (0, 0))
FAR_ODD = ((2, 1), (2, 3), (1, 1), (3, 3), (1, 3), (3, 1), (0, 1), (0, 3))


def remote(src, dst, send, recv, device):
    return pltpu.make_async_remote_copy(
        src_ref=src, dst_ref=dst, send_sem=send, recv_sem=recv, device_id=device, device_id_type=MESH
    )


def hop(step, even, core):
    dz = jnp.where(even, FAR_EVEN[step][0], FAR_ODD[step][0])
    dx = jnp.where(even, FAR_EVEN[step][1], FAR_ODD[step][1])
    return jnp.where(core == 0, dz, (4 - dz) % 4), jnp.where(core == 0, dx, (4 - dx) % 4)


def log1p_small(u):
    series = u * (1 - u * (1 / 2 - u * (1 / 3 - u * (1 / 4 - u * (1 / 5 - u * (1 / 6))))))
    return jnp.where(u < 0.05, series, jnp.log(1.0 + u))


def one_minus_exp(z):
    series = 1.0 + z * (1 / 7)
    for n in (6, 5, 4, 3, 2):
        series = 1.0 + z * series * (1 / n)
    return jnp.where(z > -0.5, -z * series, 1.0 - jnp.exp(z))


def sigmoid(v):
    return 1.0 / (1.0 + jnp.exp(-v))


def whole_kernel(
    m_rows, g_proj, i_proj, i_gates, d_gates, op, x_rows, eg, eu, ed, sg, su, sd,
    m_gain_h, taps_h, offset_h, mscale_h, x_gain_h, ids_h, weights_h, escale_h,
    out_m, out_e,
    m_gain, taps, offset, mscale, x_gain, ids, weights, escale,
    nx, nm, proj, bgates, send_x, send_n, w_sh, br, tail, edge, halo, gate, acum, loc, cm, sh, mix_hi, mix_lo,
    rows, w_in, w_dn, s_dn, o_pr, sh2, gts, carries, acc, hid, res, back,
    m_part, m_send, m_recv, m_sum, m_other, e_part, e_recv, e_sum,
    d_s, d_r, f_s, f_r, c_s, c_r, p_s, p_r, l_s, r_s, r_r, ms_s, ms_r, es_s, es_r, x_s, x_r, h_s, h_r,
):
    f32, bf16 = jnp.float32, jnp.bfloat16
    p = lax.axis_index("ep")
    t = lax.axis_index("tp")
    y = t // 2
    c = t % 2
    o = 1 - c
    z = p // 4
    x = p % 4
    par = p % 2
    half = p // 2
    partner = (p, 2 * y + o)

    def dot(a, b):
        return jnp.dot(a, b, preferred_element_type=f32)

    def wide(at):
        return pl.ds(pl.multiple_of(at * 2048, 2048), 2048)

    def local(src, dst, n):
        return pltpu.make_async_copy(src, dst, l_s.at[n])

    early = [local(m_rows.at[240:256], tail, 1), local(i_proj, proj.at[1], 2)]
    first = [local(x_rows.at[:, 1024 * q : 1024 * q + 1024], nx.at[q], 0) for q in range(4)]
    second = [local(m_rows, nm, 3), local(g_proj, proj.at[0], 4)]
    gates_in = [local(i_gates, bgates.at[0], 5), local(d_gates, bgates.at[1], 6)]
    own_w = [
        local(eg, w_in.at[:, 0:128], 7),
        local(eu, w_in.at[:, 128:256], 8),
        local(ed, w_dn.at[0:128], 9),
    ]
    own_o = local(op.at[:, wide(c)], o_pr.at[0], 10)
    own_s = [
        local(sd.at[:, wide(c)], s_dn.at[0], 11),
        local(sg, w_sh.at[:, 0:128], 12),
        local(su, w_sh.at[:, 128:256], 13),
    ]
    small = [local(ids_h, ids, 14), local(weights_h, weights, 15), local(x_gain_h, x_gain, 16)]
    small += [local(m_gain_h, m_gain, 17), local(taps_h, taps, 18), local(offset_h, offset, 19)]
    small += [local(mscale_h, mscale, 20), local(escale_h, escale, 21)]
    for copy in small[:1] + first + small[1:]:
        copy.start()

    barrier = pltpu.get_barrier_semaphore()

    def greet(k, _):
        other = (p * 2 + c + k) % 32
        pl.semaphore_signal(
            barrier, inc=1, device_id=(other // 2, 2 * y + other % 2), device_id_type=MESH
        )
        return 0

    lax.fori_loop(1, 32, greet, 0)
    for k in range(1, 4):
        pl.semaphore_signal(
            barrier, inc=1, device_id=(p, 2 * ((y + k) % 4) + c), device_id_type=MESH
        )

    small[0].wait()

    def await_recv(group, sem):
        remote(group, group, h_s.at[0], sem, partner).wait_recv()

    def await_send(group, sem):
        remote(group, group, sem, h_r.at[0], partner).wait_send()

    id0, id1 = ids[0:1, :], ids[1:2, :]
    expert = lax.broadcasted_iota(jnp.int32, (16, 256), 0)
    named0, named1 = id0 == expert, id1 == expert
    either = jnp.where(jnp.logical_or(named0, named1), 1.0, 0.0).astype(bf16)
    ahead = jnp.where(
        lax.broadcasted_iota(jnp.int32, (256, 256), 0) < lax.broadcasted_iota(jnp.int32, (256, 256), 1),
        1.0,
        0.0,
    ).astype(bf16)
    place = dot(either, ahead)
    slot0 = id0.astype(f32) * 48.0 + jnp.sum(jnp.where(named0, place, 0.0), axis=0, keepdims=True)
    slot1 = id1.astype(f32) * 48.0 + jnp.sum(jnp.where(named1, place, 0.0), axis=0, keepdims=True)

    def picked(i):
        line = ((2 * i + c) * 48 + lax.broadcasted_iota(jnp.int32, (48, 256), 0)).astype(f32)
        return jnp.where(jnp.logical_or(slot0 == line, slot1 == line), 1.0, 0.0).astype(bf16)

    chosen = jnp.concatenate([picked(i) for i in range(8)], axis=0)

    local(nx, nx, 0).wait()
    for copy in small[1:]:
        copy.wait()
    for copy in early + second + gates_in:
        copy.start()

    def norm_x(r, _):
        at = pl.ds(pl.multiple_of(r * 32, 32), 32)
        parts = [nx[q, at, :].astype(f32) for q in range(4)]
        square = sum(jnp.sum(v * v, axis=1, keepdims=True) for v in parts)
        scale = lax.rsqrt(square / 4096.0 + eps)
        for q in range(4):
            nx[q, at, :] = (parts[q] * scale * x_gain[:, 1024 * q : 1024 * q + 1024]).astype(bf16)
        return 0

    def dispatch(step, j):
        dz, dx = hop(step, par == c, c)
        e = ((z + dz) % 4) * 4 + (x + dx) % 4
        source = send_x.at[j, e // 2] if j < 2 else send_n.at[j - 2, step - FAR]
        shift = (0, 2, 1, 3)[j]
        return remote(
            source, rows.at[(y + shift) % 4, step], d_s.at[j // 2], d_r.at[landing(step, j)],
            (e, 2 * y + 1 - par),
        )

    def landing(step, j):
        if j == 0:
            return min(step, FAR)
        return FAR + (1 + step // 4 if j == 1 else 1 + j)

    def group(low, high, j):
        shift = (0, 2, 1, 3)[j]
        await_recv(rows.at[(y + shift) % 4, low:high], d_r.at[landing(low, j)])

    def gather(j):
        send_x[j] = dot(chosen, nx[(y + 2 * j) % 4]).astype(bf16).reshape(8, 48, 1024)

    lax.fori_loop(0, 8, norm_x, 0)
    gather(0)
    pl.semaphore_wait(barrier, 34)
    for step in range(4):
        dispatch(step, 0).start()
    gather(1)
    for step in range(4):
        dispatch(step, 1).start()

    for copy in early:
        copy.wait()
    v = tail[...].astype(f32)
    tail_factor = lax.rsqrt(jnp.sum(v * v, axis=1, keepdims=True) / 4096.0 + eps)
    edge[...] = dot((v * tail_factor * m_gain[...]).astype(bf16), proj[1]).astype(bf16)
    give_halo = remote(edge, halo, h_s.at[0], h_r.at[0], ((p + 1) % 16, t))
    give_halo.start()
    for j in range(2):
        for step in range(4, FAR):
            dispatch(step, j).start()

    near = []
    for step in range(FAR, 8):
        dz, dx = hop(step, par == c, c)
        near.append((((z + dz) % 4) * 4 + (x + dx) % 4) // 2)
    near_chosen = jnp.concatenate([picked(i) for i in near], axis=0)
    for j in range(2):
        send_n[j] = dot(near_chosen, nx[(y + 1 + 2 * j) % 4]).astype(bf16).reshape(8 - FAR, 48, 1024)
    for j in range(4):
        for step in range(FAR, 8):
            dispatch(step, j).start()

    swaps = [
        remote(sh, sh2, p_s.at[0], p_r.at[0], partner),
        remote(op.at[:, wide(o)], o_pr.at[1], p_s.at[1], p_r.at[1], partner),
        remote(eg, w_in.at[:, 256:384], p_s.at[2], p_r.at[2], partner),
        remote(eu, w_in.at[:, 384:512], p_s.at[3], p_r.at[3], partner),
        remote(ed, w_dn.at[128:256], p_s.at[4], p_r.at[4], partner),
        remote(sd.at[:, wide(o)], s_dn.at[1], p_s.at[5], p_r.at[5], partner),
        remote(gts.at[0], gts.at[1], p_s.at[6], p_r.at[6], partner),
    ]
    for copy in swaps[2:5] + own_w + [swaps[1], own_o, swaps[5]] + own_s:
        copy.start()

    def forward(i, d):
        return remote(
            rows.at[y, i], rows.at[y, i], f_s.at[0], f_r.at[i // 4, d],
            (p, 2 * ((y + 1 + 2 * d) % 4) + c),
        )

    def relay(step):
        group(step, step + 1, 0)
        forward(step, 0).start()
        forward(step, 1).start()

    second[0].wait()

    def norm_m(r, _):
        at = pl.ds(pl.multiple_of(r * 32, 32), 32)
        v = nm[at, :].astype(f32)
        scale = lax.rsqrt(jnp.sum(v * v, axis=1, keepdims=True) / 4096.0 + eps)
        nm[at, :] = (v * scale * m_gain[...]).astype(bf16)
        return 0

    lax.fori_loop(0, 8, norm_m, 0)

    def project(n, _):
        cols = pl.ds(pl.multiple_of(n * 256, 256), 256)
        br[:, cols] = dot(nm[...], proj[1, :, cols]).astype(bf16)
        return 0

    lax.fori_loop(0, 2, project, 0)
    second[1].wait()

    def gates(n, _):
        cols = pl.ds(pl.multiple_of(n * 256, 256), 256)
        v = dot(nm[...], proj[0, :, cols])
        gate[:, cols] = 0.5 * v * (1.0 + jnp.tanh(0.7978845608028654 * (v + 0.044715 * (v * v * v))))
        return 0

    relay(0)
    relay(1)
    gates(0, 0)
    relay(2)
    gates(1, 0)
    relay(3)
    for copy in gates_in:
        copy.wait()
    give_halo.wait_recv()

    row = lax.broadcasted_iota(jnp.int32, (256, 128), 0)

    def recur(b, _):
        cols = pl.ds(pl.multiple_of(b * 256, 256), 256)
        before = jnp.where(p == 0, 0.0, halo[:, cols].astype(f32))
        ext = jnp.concatenate([before, br[:, cols].astype(f32)], axis=0)
        tap = taps[:, cols]
        conv = tap[0:1] * pltpu.roll(ext, 3, 0)[16:]
        for k in range(1, 4):
            conv = conv + tap[k : k + 1] * (pltpu.roll(ext, 3 - k, 0) if k < 3 else ext)[16:]
        conv_out = conv.astype(bf16)
        gi = sigmoid(dot(conv_out, bgates[0, b]))
        gd = sigmoid(dot(conv_out, bgates[1, b]))
        off = offset[:, cols]
        soft = jnp.maximum(-off, 0.0) + log1p_small(jnp.exp(-jnp.abs(off)))
        log_decay = -lru_power * gd * soft
        scale = jnp.sqrt(one_minus_exp(2.0 * log_decay))
        first_row = jnp.logical_and(lax.broadcasted_iota(jnp.int32, (256, 256), 0) == 0, p == 0)
        scale = jnp.where(first_row, 1.0, scale)
        loc[:, cols] = scale * gi * conv_out.astype(f32)
        acum[:, cols] = jnp.exp(log_decay)
        return 0

    recur(0, 0)
    relay(4)
    recur(1, 0)
    relay(5)

    def scan(b, _):
        cols = pl.ds(pl.multiple_of(b * 128, 128), 128)
        av, bv = acum[:, cols], loc[:, cols]
        for d in (1, 2, 4, 8, 16, 32, 64, 128):
            if d < 8:
                a_up = jnp.where(row < d, 1.0, pltpu.roll(av, d, 0))
                b_up = jnp.where(row < d, 0.0, pltpu.roll(bv, d, 0))
            else:
                a_up = jnp.concatenate([jnp.ones((d, 128), f32), av[: 256 - d]], axis=0)
                b_up = jnp.concatenate([jnp.zeros((d, 128), f32), bv[: 256 - d]], axis=0)
            bv = av * b_up + bv
            av = av * a_up
        acum[:, cols] = av
        loc[:, cols] = bv
        cm[pl.ds(b, 1), :] = av[255:256]
        cm[pl.ds(4 + b, 1), :] = bv[255:256]
        return 0

    lax.fori_loop(0, 4, scan, 0)

    def carry(k):
        return remote(cm, carries.at[k - 1], c_s.at[0], c_r.at[0], ((p + k) % 16, t))

    def carry_go(k, _):
        carry(k).start()
        return 0

    lax.fori_loop(1, 16, carry_go, 0)
    line = lax.broadcasted_iota(jnp.int32, (128, 256), 0)
    tile = jnp.where(
        line == 0, slot0,
        jnp.where(line == 1, slot1, jnp.where(line == 2, weights[0:1, :], jnp.where(line == 3, weights[1:2, :], 0.0))),
    )
    turned = tile.T
    every = lax.broadcasted_iota(jnp.int32, (256, 768), 1).astype(f32)
    mixing = jnp.where(turned[:, 0:1] == every, turned[:, 2:3], 0.0) + jnp.where(
        turned[:, 1:2] == every, turned[:, 3:4], 0.0
    )
    high = mixing.astype(bf16)
    mix_hi[...] = high
    mix_lo[...] = (mixing - high.astype(f32)).astype(bf16)

    for copy in own_s:
        copy.wait()
    shared = dot(nx[0], w_sh[0:1024, :])
    for q in range(1, 4):
        shared = shared + dot(nx[q], w_sh[1024 * q : 1024 * q + 1024, :])
    g, u = shared[:, 0:128], shared[:, 128:256]
    sh[...] = (g / (1.0 + jnp.exp(-g)) * u).astype(bf16)
    swaps[0].start()

    def scatter(part, recv, send_sem, recv_sem, ch):
        return [
            remote(
                part.at[ch, (y + k) % 4], recv.at[ch, k - 1], send_sem.at[0],
                recv_sem.at[0], (p, 2 * ((y + k) % 4) + c),
            )
            for k in range(1, 4)
        ]

    def swap(total, other, base, ch):
        return remote(
            total.at[ch, o], other.at[ch], x_s.at[0], x_r.at[0], partner
        )

    def settle(part, sent, recv, total, other, send_sem, recv_sem, base):
        await_recv(recv, recv_sem.at[0])

        def one(ch, _):
            value = part[ch, y] + sum(recv[ch, k].astype(f32) for k in range(3))
            total[ch] = value.reshape(2, 32, CW)
            swap(total, other, base, ch).start()
            return 0

        lax.fori_loop(0, NCH, one, 0)

    def finish(total, other, scale, out, base):
        square = jnp.zeros((32, 1), f32)
        await_recv(other, x_r.at[0])
        for ch in range(NCH):
            mine, theirs = total[ch, c], other[ch]
            square += jnp.sum(mine * mine + theirs * theirs, axis=1, keepdims=True)
        level = lax.rsqrt(square / 4096.0 + eps)
        for ch in range(NCH):
            for values, side in ((total[ch, c], c), (other[ch], o)):
                cols = pl.ds(pl.multiple_of(side * 2048 + ch * CW, CW), CW)
                out[:, cols] = (values * level * scale[:, cols]).astype(bf16)

    for copy in own_w:
        copy.wait()
    for copy in swaps[2:5]:
        copy.wait_recv()

    def hidden(half_of):
        at = slice(192 * half_of, 192 * half_of + 192)

        def quarter(q):
            depth = pl.ds(pl.multiple_of(q * 1024, 1024), 1024)
            block = rows[q, 4 * half_of : 4 * half_of + 4].reshape(192, 1024)
            return dot(block, w_in[depth, :])

        if half_of == 1:
            group(FAR, 8, 0)
        acc[at] = quarter(y)
        group(4 * half_of, 4 * half_of + 4, 1)
        acc[at] += quarter((y + 2) % 4)
        for d in range(2):
            source = (y + 3 + 2 * d) % 4
            await_recv(rows.at[source, 4 * half_of : min(FAR, 4 * half_of + 4)], f_r.at[half_of, d])
            if half_of == 1:
                group(FAR, 8, 3 - d)
            acc[at] += quarter(source)
        for side in range(2):
            g = acc[at, 256 * side : 256 * side + 128]
            u = acc[at, 256 * side + 128 : 256 * side + 256]
            hid[at, 128 * side : 128 * side + 128] = (g / (1.0 + jnp.exp(-g)) * u).astype(bf16)

    def returning(ch, step, h):
        dz, dx = hop(step, par == o, par)
        s = ((z + 4 - dz) % 4) * 4 + (x + 4 - dx) % 4
        return s, remote(
            res.at[ch, h, step], back.at[ch, p], r_s.at[ch], r_r.at[ch], (s, 2 * y + h)
        )

    def give(low, high):
        def one(ch, _):
            for h in range(2):
                cols = pl.ds(pl.multiple_of(h * 2048 + ch * CW, CW), CW)
                res[ch, h, low:high] = (
                    dot(hid[48 * low : 48 * high], w_dn[:, cols]).astype(bf16).reshape(high - low, 48, CW)
                )
            for h in range(2):
                for step in range(low, high):
                    s, copy = returning(ch, step, h)
                    if step < 7:
                        copy.start()
                    else:

                        @pl.when(jnp.logical_or(s != p, c != h))
                        def _():
                            copy.start()

                        @pl.when(jnp.logical_and(s == p, c == h))
                        def _():
                            back[ch, p] = res[ch, h, step]

            return 0

        return one

    hidden(0)
    lax.fori_loop(0, LEAD, give(0, 4), 0)
    hidden(1)
    lax.fori_loop(0, LEAD, give(4, 8), 0)
    lax.fori_loop(LEAD, NCH, give(0, 8), 0)

    await_recv(carries, c_r.at[0])

    def fold(n, state):
        k = 15 - n
        later = carries[k - 1]
        return jnp.where(k <= p, later[0:4] * state + later[4:8], state)

    state = lax.fori_loop(0, 15, fold, jnp.zeros((4, 128), f32))
    for j in range(4):
        cols = slice(128 * j, 128 * j + 128)
        states = loc[:, cols] + acum[:, cols] * state[j : j + 1]
        gts[0, :, cols] = (gate[:, cols] * states).astype(bf16)

    swaps[6].start()

    own_o.wait()
    swaps[1].wait_recv()
    swaps[6].wait_recv()

    def mixed(ch, _):
        cols = pl.ds(pl.multiple_of(ch * CW, CW), CW)
        m_part[ch] = (dot(gts[0], o_pr[0, :, cols]) + dot(gts[1], o_pr[1, :, cols])).reshape(4, 64, CW)
        m_send[ch] = m_part[ch].astype(bf16)
        for copy in scatter(m_send, m_recv, ms_s, ms_r, ch):
            copy.start()
        return 0

    lax.fori_loop(0, NCH, mixed, 0)

    swaps[0].wait_recv()
    swaps[5].wait_recv()

    def shared_part(ch, _):
        cols = pl.ds(pl.multiple_of(ch * CW, CW), CW)
        e_part[ch] = (dot(sh[...], s_dn[0, :, cols]) + dot(sh2[...], s_dn[1, :, cols])).reshape(4, 2, 32, CW)
        return 0

    lax.fori_loop(0, NCH, shared_part, 0)

    def final(ch):
        return [
            remote(
                e_part.at[ch, (y + k) % 4, w], e_recv.at[ch, 2 * (k - 1) + c], es_s.at[0],
                es_r.at[ch], (p, 2 * ((y + k) % 4) + w),
            )
            for k in range(1, 4)
            for w in range(2)
        ] + [remote(e_part.at[ch, y, o], e_recv.at[ch, 6], es_s.at[1], es_r.at[ch], partner)]

    def combine(ch, _):
        @pl.when(par == o)
        def _():
            await_recv(back.at[ch, 0:15], r_r.at[ch])

        @pl.when(par != o)
        def _():
            await_recv(back.at[ch], r_r.at[ch])

        returned = back[ch].reshape(768, CW)
        e_part[ch] = e_part[ch] + (
            dot(mix_hi[...], returned) + dot(mix_lo[...], returned)
        ).reshape(4, 2, 32, CW)
        for copy in final(ch):
            copy.start()
        return 0

    lax.fori_loop(0, NCH // 2, combine, 0)
    settle(m_part, m_send, m_recv, m_sum, m_other, ms_s, ms_r, 0)
    finish(m_sum, m_other, mscale, out_m, 0)
    lax.fori_loop(NCH // 2, NCH, combine, 0)
    await_send(send_x, d_s.at[0])
    await_send(send_n, d_s.at[1])
    await_send(rows.at[0:2, 0:FAR], f_s.at[0])
    await_send(carries, c_s.at[0])

    @pl.when(par == o)
    def _():
        for ch in range(NCH):
            await_send(back.at[ch, 0:15], r_s.at[ch])

    @pl.when(par != o)
    def _():
        for ch in range(NCH):
            await_send(back.at[ch], r_s.at[ch])

    await_send(m_recv, ms_s.at[0])
    await_send(m_other, x_s.at[0])
    for copy in swaps:
        copy.wait_send()
    give_halo.wait_send()

    def settle_last(ch, square):
        await_recv(e_recv.at[ch, 0:7], es_r.at[ch])
        mine = e_part[ch, y, c] + e_recv[ch, c] + e_recv[ch, 2 + c] + e_recv[ch, 4 + c]
        theirs = e_recv[ch, 6] + e_recv[ch, o] + e_recv[ch, 2 + o] + e_recv[ch, 4 + o]
        e_sum[ch, c] = mine
        e_sum[ch, o] = theirs
        return square + jnp.sum(mine * mine + theirs * theirs, axis=1, keepdims=True)

    square = lax.fori_loop(0, NCH, settle_last, jnp.zeros((32, 1), f32))
    level = lax.rsqrt(square / 4096.0 + eps)
    for ch in range(NCH):
        for w in range(2):
            cols = slice(w * 2048 + ch * CW, w * 2048 + ch * CW + CW)
            out_e[:, cols] = (e_sum[ch, w] * level * escale[:, cols]).astype(bf16)

    await_send(e_part.at[:, 1:4], es_s.at[0])
    await_send(e_part.at[:, 0, 0], es_s.at[1])


def body(
    mixer_rows, mixer_gain, gate_proj, input_proj, conv_taps, input_gates, decay_gates,
    decay_offset, out_proj, mixer_scale, expert_rows, expert_gain, route_ids, route_weights,
    expert_gate, expert_up, expert_down, shared_gate, shared_up, shared_down, expert_scale,
):
    f32, bf16 = jnp.float32, jnp.bfloat16
    dma = pltpu.SemaphoreType.DMA
    hbm = pl.BlockSpec(memory_space=pltpu.HBM)
    vmem = pl.BlockSpec(memory_space=pltpu.VMEM)
    outs = pl.pallas_call(
        whole_kernel,
        out_shape=[jax.ShapeDtypeStruct((32, 4096), bf16)] * 2,
        in_specs=[hbm] * 21,
        out_specs=[vmem] * 2,
        scratch_shapes=[
            pltpu.VMEM((1, 4096), f32),
            pltpu.VMEM((4, 512), f32),
            pltpu.VMEM((1, 512), f32),
            pltpu.VMEM((1, 4096), f32),
            pltpu.VMEM((1, 4096), f32),
            pltpu.VMEM((2, 256), jnp.int32),
            pltpu.VMEM((2, 256), f32),
            pltpu.VMEM((1, 4096), f32),
            pltpu.VMEM((4, 256, 1024), bf16),
            pltpu.VMEM((256, 4096), bf16),
            pltpu.VMEM((2, 4096, 512), bf16),
            pltpu.VMEM((2, 2, 256, 256), bf16),
            pltpu.VMEM((2, 8, 48, 1024), bf16),
            pltpu.VMEM((2, 8 - FAR, 48, 1024), bf16),
            pltpu.VMEM((4096, 256), bf16),
            pltpu.VMEM((256, 512), bf16),
            pltpu.VMEM((16, 4096), bf16),
            pltpu.VMEM((16, 512), bf16),
            pltpu.VMEM((16, 512), bf16),
            pltpu.VMEM((256, 512), f32),
            pltpu.VMEM((256, 512), f32),
            pltpu.VMEM((256, 512), f32),
            pltpu.VMEM((8, 128), f32),
            pltpu.VMEM((256, 128), bf16),
            pltpu.VMEM((256, 768), bf16),
            pltpu.VMEM((256, 768), bf16),
            pltpu.VMEM((4, 8, 48, 1024), bf16),
            pltpu.VMEM((4096, 512), bf16),
            pltpu.VMEM((256, 4096), bf16),
            pltpu.VMEM((2, 128, 2048), bf16),
            pltpu.VMEM((2, 512, 2048), bf16),
            pltpu.VMEM((256, 128), bf16),
            pltpu.VMEM((2, 256, 512), bf16),
            pltpu.VMEM((15, 8, 128), f32),
            pltpu.VMEM((384, 512), f32),
            pltpu.VMEM((384, 256), bf16),
            pltpu.VMEM((NCH, 2, 8, 48, CW), bf16),
            pltpu.VMEM((NCH, 16, 48, CW), bf16),
        ]
        + [
            pltpu.VMEM((NCH, 4, 64, CW), f32),
            pltpu.VMEM((NCH, 4, 64, CW), bf16),
            pltpu.VMEM((NCH, 3, 64, CW), bf16),
            pltpu.VMEM((NCH, 2, 32, CW), f32),
            pltpu.VMEM((NCH, 32, CW), f32),
            pltpu.VMEM((NCH, 4, 2, 32, CW), f32),
            pltpu.VMEM((NCH, 7, 32, CW), f32),
            pltpu.VMEM((NCH, 2, 32, CW), f32),
        ]
        + [
            dma((2,)), dma((FAR + 5,)), dma((1,)), dma((2, 2)), dma((1,)), dma((1,)),
            dma((7,)), dma((7,)), dma((22,)), dma((NCH,)), dma((NCH,)),
            dma((1,)), dma((1,)), dma((2,)), dma((NCH,)), dma((1,)), dma((1,)), dma((1,)), dma((1,)),
        ],
        compiler_params=pltpu.CompilerParams(
            collective_id=0, has_side_effects=True, vmem_limit_bytes=67043328
        ),
    )(
        mixer_rows, gate_proj, input_proj, input_gates, decay_gates, out_proj, expert_rows,
        expert_gate[0], expert_up[0], expert_down[0], shared_gate, shared_up, shared_down,
        mixer_gain[None, :], conv_taps, decay_offset[None, :], mixer_scale[None, :],
        expert_gain[None, :], route_ids.T, route_weights.T, expert_scale[None, :],
    )

    def hand_out(a, b, a_out, b_out):
        a_out[...] = a[...]
        b_out[...] = b[...]

    return tuple(
        pl.pallas_call(
            hand_out,
            out_shape=[jax.ShapeDtypeStruct((32, 4096), bf16)] * 2,
            in_specs=[vmem] * 2,
            out_specs=[vmem] * 2,
        )(*outs)
    )


def solution(mesh):
    placed = (
        P("ep", None),
        P(),
        P(None, "tp"),
        P(None, "tp"),
        P(None, "tp"),
        P("tp", None, None),
        P("tp", None, None),
        P("tp"),
        P("tp", None),
        P(),
        P("ep", None),
        P(),
        P("ep", None),
        P("ep", None),
        P("ep", None, "tp"),
        P("ep", None, "tp"),
        P("ep", "tp", None),
        P(None, "tp"),
        P(None, "tp"),
        P("tp", None),
        P(),
    )
    return jax.shard_map(
        body,
        mesh=mesh,
        in_specs=placed,
        out_specs=(P(("ep", "tp"), None), P(("ep", "tp"), None)),
        check_vma=False,
    )
```

```python
import jax
import jax.numpy as jnp
from jax import lax
from jax.experimental import pallas as pl
from jax.experimental.pallas import tpu as pltpu
from jax.sharding import PartitionSpec as P

eps = 1e-06
lru_power = 8.0


MESH = pl.DeviceIdType.MESH
NCH = 4
FAR = 7
LEAD = 1
CW = 2048 // NCH
FAR_EVEN = ((2, 2), (1, 2), (3, 2), (2, 0), (0, 2), (1, 0), (3, 0), (0, 0))
FAR_ODD = ((2, 1), (2, 3), (1, 1), (3, 3), (1, 3), (3, 1), (0, 1), (0, 3))


def remote(src, dst, send, recv, device):
    return pltpu.make_async_remote_copy(
        src_ref=src, dst_ref=dst, send_sem=send, recv_sem=recv, device_id=device, device_id_type=MESH
    )


def hop(step, even, core):
    dz = jnp.where(even, FAR_EVEN[step][0], FAR_ODD[step][0])
    dx = jnp.where(even, FAR_EVEN[step][1], FAR_ODD[step][1])
    return jnp.where(core == 0, dz, (4 - dz) % 4), jnp.where(core == 0, dx, (4 - dx) % 4)


def log1p_small(u):
    series = u * (1 - u * (1 / 2 - u * (1 / 3 - u * (1 / 4 - u * (1 / 5 - u * (1 / 6))))))
    return jnp.where(u < 0.05, series, jnp.log(1.0 + u))


def one_minus_exp(z):
    series = 1.0 + z * (1 / 7)
    for n in (6, 5, 4, 3, 2):
        series = 1.0 + z * series * (1 / n)
    return jnp.where(z > -0.5, -z * series, 1.0 - jnp.exp(z))


def sigmoid(v):
    return 1.0 / (1.0 + jnp.exp(-v))


def whole_kernel(
    m_rows, g_proj, i_proj, i_gates, d_gates, op, x_rows, eg, eu, ed, sg, su, sd,
    m_gain_h, taps_h, offset_h, mscale_h, x_gain_h, ids_h, weights_h, escale_h,
    out_m, out_e,
    m_gain, taps, offset, mscale, x_gain, ids, weights, escale,
    nx, nm, proj, bgates, send_x, send_n, w_sh, br, tail, edge, halo, gate, acum, loc, cm, sh, mix_hi, mix_lo,
    rows, w_in, w_dn, s_dn, o_pr, sh2, gts, carries, acc, hid, res, back,
    m_part, m_send, m_recv, m_sum, m_other, e_part, e_recv, e_sum,
    d_s, d_r, f_s, f_r, c_s, c_r, p_s, p_r, l_s, r_s, r_r, ms_s, ms_r, es_s, es_r, x_s, x_r, h_s, h_r,
):
    f32, bf16 = jnp.float32, jnp.bfloat16
    p = lax.axis_index("ep")
    t = lax.axis_index("tp")
    y = t // 2
    c = t % 2
    o = 1 - c
    z = p // 4
    x = p % 4
    par = p % 2
    half = p // 2
    partner = (p, 2 * y + o)

    def dot(a, b):
        return jnp.dot(a, b, preferred_element_type=f32)

    def wide(at):
        return pl.ds(pl.multiple_of(at * 2048, 2048), 2048)

    def local(src, dst, n):
        return pltpu.make_async_copy(src, dst, l_s.at[n])

    early = [local(m_rows.at[240:256], tail, 1), local(i_proj, proj.at[1], 2)]
    first = [
        local(
            x_rows.at[r : r + 128, 1024 * q : 1024 * q + 1024], nx.at[q, r : r + 128], 22 if r else 0
        )
        for r in (0, 128)
        for q in range(4)
    ]
    second = [local(m_rows, nm, 3), local(g_proj, proj.at[0], 4)]
    gates_in = [local(i_gates, bgates.at[0], 5), local(d_gates, bgates.at[1], 6)]
    own_w = [
        local(eg, w_in.at[:, 0:128], 7),
        local(eu, w_in.at[:, 128:256], 8),
        local(ed, w_dn.at[0:128], 9),
    ]
    own_o = local(op.at[:, wide(c)], o_pr.at[0], 10)
    own_s = [
        local(sd.at[:, wide(c)], s_dn.at[0], 11),
        local(sg, w_sh.at[:, 0:128], 12),
        local(su, w_sh.at[:, 128:256], 13),
    ]
    small = [local(ids_h, ids, 14), local(weights_h, weights, 15), local(x_gain_h, x_gain, 16)]
    small += [local(m_gain_h, m_gain, 17), local(taps_h, taps, 18), local(offset_h, offset, 19)]
    small += [local(mscale_h, mscale, 20), local(escale_h, escale, 21)]
    for copy in small[:1] + first + small[1:]:
        copy.start()

    barrier = pltpu.get_barrier_semaphore()

    def greet(k, _):
        other = (p * 2 + c + k) % 32
        pl.semaphore_signal(
            barrier, inc=1, device_id=(other // 2, 2 * y + other % 2), device_id_type=MESH
        )
        return 0

    lax.fori_loop(1, 32, greet, 0)
    for k in range(1, 4):
        pl.semaphore_signal(
            barrier, inc=1, device_id=(p, 2 * ((y + k) % 4) + c), device_id_type=MESH
        )

    small[0].wait()

    def await_recv(group, sem):
        remote(group, group, h_s.at[0], sem, partner).wait_recv()

    def await_send(group, sem):
        remote(group, group, sem, h_r.at[0], partner).wait_send()

    id0, id1 = ids[0:1, :], ids[1:2, :]
    expert = lax.broadcasted_iota(jnp.int32, (16, 256), 0)
    named0, named1 = id0 == expert, id1 == expert
    either = jnp.where(jnp.logical_or(named0, named1), 1.0, 0.0).astype(bf16)
    ahead = jnp.where(
        lax.broadcasted_iota(jnp.int32, (256, 256), 0) < lax.broadcasted_iota(jnp.int32, (256, 256), 1),
        1.0,
        0.0,
    ).astype(bf16)
    place = dot(either, ahead)
    slot0 = id0.astype(f32) * 48.0 + jnp.sum(jnp.where(named0, place, 0.0), axis=0, keepdims=True)
    slot1 = id1.astype(f32) * 48.0 + jnp.sum(jnp.where(named1, place, 0.0), axis=0, keepdims=True)

    def picked(i):
        line = ((2 * i + c) * 48 + lax.broadcasted_iota(jnp.int32, (48, 256), 0)).astype(f32)
        return jnp.where(jnp.logical_or(slot0 == line, slot1 == line), 1.0, 0.0).astype(bf16)

    chosen = jnp.concatenate([picked(i) for i in range(8)], axis=0)

    for copy in small[1:]:
        copy.wait()

    def norm_x(r, _):
        at = pl.ds(pl.multiple_of(r * 32, 32), 32)
        parts = [nx[q, at, :].astype(f32) for q in range(4)]
        square = sum(jnp.sum(v * v, axis=1, keepdims=True) for v in parts)
        scale = lax.rsqrt(square / 4096.0 + eps)
        for q in range(4):
            nx[q, at, :] = (parts[q] * scale * x_gain[:, 1024 * q : 1024 * q + 1024]).astype(bf16)
        return 0

    def dispatch(step, j):
        dz, dx = hop(step, par == c, c)
        e = ((z + dz) % 4) * 4 + (x + dx) % 4
        source = send_x.at[j, e // 2] if j < 2 else send_n.at[j - 2, step - FAR]
        shift = (0, 2, 1, 3)[j]
        return remote(
            source, rows.at[(y + shift) % 4, step], d_s.at[j // 2], d_r.at[landing(step, j)],
            (e, 2 * y + 1 - par),
        )

    def landing(step, j):
        if j == 0:
            return min(step, FAR)
        return FAR + (1 + step // 4 if j == 1 else 1 + j)

    def group(low, high, j):
        shift = (0, 2, 1, 3)[j]
        await_recv(rows.at[(y + shift) % 4, low:high], d_r.at[landing(low, j)])

    def gather(j):
        send_x[j] = dot(chosen, nx[(y + 2 * j) % 4]).astype(bf16).reshape(8, 48, 1024)

    local(nx.at[:, 0:128], nx.at[:, 0:128], 0).wait()
    lax.fori_loop(0, 4, norm_x, 0)
    local(nx.at[:, 128:256], nx.at[:, 128:256], 22).wait()
    for copy in early + second + gates_in:
        copy.start()
    lax.fori_loop(4, 8, norm_x, 0)
    gather(0)
    pl.semaphore_wait(barrier, 34)
    for step in range(4):
        dispatch(step, 0).start()
    gather(1)
    for step in range(4):
        dispatch(step, 1).start()

    for copy in early:
        copy.wait()
    v = tail[...].astype(f32)
    tail_factor = lax.rsqrt(jnp.sum(v * v, axis=1, keepdims=True) / 4096.0 + eps)
    edge[...] = dot((v * tail_factor * m_gain[...]).astype(bf16), proj[1]).astype(bf16)
    give_halo = remote(edge, halo, h_s.at[0], h_r.at[0], ((p + 1) % 16, t))
    give_halo.start()
    for j in range(2):
        for step in range(4, FAR):
            dispatch(step, j).start()

    near = []
    for step in range(FAR, 8):
        dz, dx = hop(step, par == c, c)
        near.append((((z + dz) % 4) * 4 + (x + dx) % 4) // 2)
    near_chosen = jnp.concatenate([picked(i) for i in near], axis=0)
    for j in range(2):
        send_n[j] = dot(near_chosen, nx[(y + 1 + 2 * j) % 4]).astype(bf16).reshape(8 - FAR, 48, 1024)
    for j in range(4):
        for step in range(FAR, 8):
            dispatch(step, j).start()

    swaps = [
        remote(sh, sh2, p_s.at[0], p_r.at[0], partner),
        remote(op.at[:, wide(o)], o_pr.at[1], p_s.at[1], p_r.at[1], partner),
        remote(eg, w_in.at[:, 256:384], p_s.at[2], p_r.at[2], partner),
        remote(eu, w_in.at[:, 384:512], p_s.at[3], p_r.at[3], partner),
        remote(ed, w_dn.at[128:256], p_s.at[4], p_r.at[4], partner),
        remote(sd.at[:, wide(o)], s_dn.at[1], p_s.at[5], p_r.at[5], partner),
        remote(gts.at[0], gts.at[1], p_s.at[6], p_r.at[6], partner),
    ]
    for copy in swaps[2:5] + own_w + [swaps[1], own_o, swaps[5]] + own_s:
        copy.start()

    def forward(i, d):
        return remote(
            rows.at[y, i], rows.at[y, i], f_s.at[0], f_r.at[i // 4, d],
            (p, 2 * ((y + 1 + 2 * d) % 4) + c),
        )

    def relay(step):
        group(step, step + 1, 0)
        forward(step, 0).start()
        forward(step, 1).start()

    second[0].wait()

    def norm_m(r, _):
        at = pl.ds(pl.multiple_of(r * 32, 32), 32)
        v = nm[at, :].astype(f32)
        scale = lax.rsqrt(jnp.sum(v * v, axis=1, keepdims=True) / 4096.0 + eps)
        nm[at, :] = (v * scale * m_gain[...]).astype(bf16)
        return 0

    lax.fori_loop(0, 8, norm_m, 0)

    def project(n, _):
        cols = pl.ds(pl.multiple_of(n * 256, 256), 256)
        br[:, cols] = dot(nm[...], proj[1, :, cols]).astype(bf16)
        return 0

    lax.fori_loop(0, 2, project, 0)
    second[1].wait()

    def gates(n, _):
        cols = pl.ds(pl.multiple_of(n * 256, 256), 256)
        v = dot(nm[...], proj[0, :, cols])
        gate[:, cols] = 0.5 * v * (1.0 + jnp.tanh(0.7978845608028654 * (v + 0.044715 * (v * v * v))))
        return 0

    relay(0)
    relay(1)
    gates(0, 0)
    relay(2)
    gates(1, 0)
    relay(3)
    for copy in gates_in:
        copy.wait()
    give_halo.wait_recv()

    row = lax.broadcasted_iota(jnp.int32, (256, 128), 0)

    def recur(b, _):
        cols = pl.ds(pl.multiple_of(b * 256, 256), 256)
        before = jnp.where(p == 0, 0.0, halo[:, cols].astype(f32))
        ext = jnp.concatenate([before, br[:, cols].astype(f32)], axis=0)
        tap = taps[:, cols]
        conv = tap[0:1] * pltpu.roll(ext, 3, 0)[16:]
        for k in range(1, 4):
            conv = conv + tap[k : k + 1] * (pltpu.roll(ext, 3 - k, 0) if k < 3 else ext)[16:]
        conv_out = conv.astype(bf16)
        gi = sigmoid(dot(conv_out, bgates[0, b]))
        gd = sigmoid(dot(conv_out, bgates[1, b]))
        off = offset[:, cols]
        soft = jnp.maximum(-off, 0.0) + log1p_small(jnp.exp(-jnp.abs(off)))
        log_decay = -lru_power * gd * soft
        scale = jnp.sqrt(one_minus_exp(2.0 * log_decay))
        first_row = jnp.logical_and(lax.broadcasted_iota(jnp.int32, (256, 256), 0) == 0, p == 0)
        scale = jnp.where(first_row, 1.0, scale)
        loc[:, cols] = scale * gi * conv_out.astype(f32)
        acum[:, cols] = jnp.exp(log_decay)
        return 0

    recur(0, 0)
    relay(4)
    recur(1, 0)
    relay(5)
    relay(6)

    def scan(b, _):
        cols = pl.ds(pl.multiple_of(b * 128, 128), 128)
        av, bv = acum[:, cols], loc[:, cols]
        for d in (1, 2, 4, 8, 16, 32, 64, 128):
            if d < 8:
                a_up = jnp.where(row < d, 1.0, pltpu.roll(av, d, 0))
                b_up = jnp.where(row < d, 0.0, pltpu.roll(bv, d, 0))
            else:
                a_up = jnp.concatenate([jnp.ones((d, 128), f32), av[: 256 - d]], axis=0)
                b_up = jnp.concatenate([jnp.zeros((d, 128), f32), bv[: 256 - d]], axis=0)
            bv = av * b_up + bv
            av = av * a_up
        acum[:, cols] = av
        loc[:, cols] = bv
        cm[pl.ds(b, 1), :] = av[255:256]
        cm[pl.ds(4 + b, 1), :] = bv[255:256]
        return 0

    lax.fori_loop(0, 4, scan, 0)

    def carry(k):
        return remote(cm, carries.at[k - 1], c_s.at[0], c_r.at[0], ((p + k) % 16, t))

    def carry_go(k, _):
        carry(k).start()
        return 0

    lax.fori_loop(1, 16, carry_go, 0)
    line = lax.broadcasted_iota(jnp.int32, (128, 256), 0)
    tile = jnp.where(
        line == 0, slot0,
        jnp.where(line == 1, slot1, jnp.where(line == 2, weights[0:1, :], jnp.where(line == 3, weights[1:2, :], 0.0))),
    )
    turned = tile.T
    every = lax.broadcasted_iota(jnp.int32, (256, 768), 1).astype(f32)
    mixing = jnp.where(turned[:, 0:1] == every, turned[:, 2:3], 0.0) + jnp.where(
        turned[:, 1:2] == every, turned[:, 3:4], 0.0
    )
    high = mixing.astype(bf16)
    mix_hi[...] = high
    mix_lo[...] = (mixing - high.astype(f32)).astype(bf16)

    for copy in own_s:
        copy.wait()
    shared = dot(nx[0], w_sh[0:1024, :])
    for q in range(1, 4):
        shared = shared + dot(nx[q], w_sh[1024 * q : 1024 * q + 1024, :])
    g, u = shared[:, 0:128], shared[:, 128:256]
    sh[...] = (g / (1.0 + jnp.exp(-g)) * u).astype(bf16)
    swaps[0].start()

    def scatter(part, recv, send_sem, recv_sem, ch):
        return [
            remote(
                part.at[ch, (y + k) % 4], recv.at[ch, k - 1], send_sem.at[0],
                recv_sem.at[0], (p, 2 * ((y + k) % 4) + c),
            )
            for k in range(1, 4)
        ]

    def swap(total, other, base, ch):
        return remote(
            total.at[ch, o], other.at[ch], x_s.at[0], x_r.at[0], partner
        )

    def settle(part, sent, recv, total, other, send_sem, recv_sem, base):
        await_recv(recv, recv_sem.at[0])

        def one(ch, _):
            value = part[ch, y] + sum(recv[ch, k].astype(f32) for k in range(3))
            total[ch] = value.reshape(2, 32, CW)
            swap(total, other, base, ch).start()
            return 0

        lax.fori_loop(0, NCH, one, 0)

    def finish(total, other, scale, out, base):
        square = jnp.zeros((32, 1), f32)
        await_recv(other, x_r.at[0])
        for ch in range(NCH):
            mine, theirs = total[ch, c], other[ch]
            square += jnp.sum(mine * mine + theirs * theirs, axis=1, keepdims=True)
        level = lax.rsqrt(square / 4096.0 + eps)
        for ch in range(NCH):
            for values, side in ((total[ch, c], c), (other[ch], o)):
                cols = pl.ds(pl.multiple_of(side * 2048 + ch * CW, CW), CW)
                out[:, cols] = (values * level * scale[:, cols]).astype(bf16)

    for copy in own_w:
        copy.wait()
    for copy in swaps[2:5]:
        copy.wait_recv()

    def hidden(half_of):
        at = slice(192 * half_of, 192 * half_of + 192)

        def quarter(q):
            depth = pl.ds(pl.multiple_of(q * 1024, 1024), 1024)
            block = rows[q, 4 * half_of : 4 * half_of + 4].reshape(192, 1024)
            return dot(block, w_in[depth, :])

        if half_of == 1:
            group(FAR, 8, 0)
        acc[at] = quarter(y)
        group(4 * half_of, 4 * half_of + 4, 1)
        acc[at] += quarter((y + 2) % 4)
        for d in range(2):
            source = (y + 3 + 2 * d) % 4
            await_recv(rows.at[source, 4 * half_of : min(FAR, 4 * half_of + 4)], f_r.at[half_of, d])
            if half_of == 1:
                group(FAR, 8, 3 - d)
            acc[at] += quarter(source)
        for side in range(2):
            g = acc[at, 256 * side : 256 * side + 128]
            u = acc[at, 256 * side + 128 : 256 * side + 256]
            hid[at, 128 * side : 128 * side + 128] = (g / (1.0 + jnp.exp(-g)) * u).astype(bf16)

    def returning(ch, step, h):
        dz, dx = hop(step, par == o, par)
        s = ((z + 4 - dz) % 4) * 4 + (x + 4 - dx) % 4
        return s, remote(
            res.at[ch, h, step], back.at[ch, p], r_s.at[ch], r_r.at[ch], (s, 2 * y + h)
        )

    def give(low, high):
        def one(ch, _):
            for h in range(2):
                cols = pl.ds(pl.multiple_of(h * 2048 + ch * CW, CW), CW)
                res[ch, h, low:high] = (
                    dot(hid[48 * low : 48 * high], w_dn[:, cols]).astype(bf16).reshape(high - low, 48, CW)
                )
            for h in range(2):
                for step in range(low, high):
                    s, copy = returning(ch, step, h)
                    if step < 7:
                        copy.start()
                    else:

                        @pl.when(jnp.logical_or(s != p, c != h))
                        def _():
                            copy.start()

                        @pl.when(jnp.logical_and(s == p, c == h))
                        def _():
                            back[ch, p] = res[ch, h, step]

            return 0

        return one

    hidden(0)
    lax.fori_loop(0, LEAD, give(0, 4), 0)
    hidden(1)
    lax.fori_loop(0, LEAD, give(4, 8), 0)
    lax.fori_loop(LEAD, NCH, give(0, 8), 0)

    await_recv(carries, c_r.at[0])

    def fold(n, state):
        k = 15 - n
        later = carries[k - 1]
        return jnp.where(k <= p, later[0:4] * state + later[4:8], state)

    state = lax.fori_loop(0, 15, fold, jnp.zeros((4, 128), f32))
    for j in range(4):
        cols = slice(128 * j, 128 * j + 128)
        states = loc[:, cols] + acum[:, cols] * state[j : j + 1]
        gts[0, :, cols] = (gate[:, cols] * states).astype(bf16)

    swaps[6].start()

    own_o.wait()
    swaps[1].wait_recv()
    swaps[6].wait_recv()

    def mixed(ch, _):
        cols = pl.ds(pl.multiple_of(ch * CW, CW), CW)
        m_part[ch] = (dot(gts[0], o_pr[0, :, cols]) + dot(gts[1], o_pr[1, :, cols])).reshape(4, 64, CW)
        m_send[ch] = m_part[ch].astype(bf16)
        for copy in scatter(m_send, m_recv, ms_s, ms_r, ch):
            copy.start()
        return 0

    lax.fori_loop(0, NCH, mixed, 0)

    swaps[0].wait_recv()
    swaps[5].wait_recv()

    def shared_part(ch, _):
        cols = pl.ds(pl.multiple_of(ch * CW, CW), CW)
        e_part[ch] = (dot(sh[...], s_dn[0, :, cols]) + dot(sh2[...], s_dn[1, :, cols])).reshape(4, 2, 32, CW)
        return 0

    lax.fori_loop(0, NCH, shared_part, 0)

    def final(ch):
        return [
            remote(
                e_part.at[ch, (y + k) % 4, w], e_recv.at[ch, 2 * (k - 1) + c], es_s.at[0],
                es_r.at[ch], (p, 2 * ((y + k) % 4) + w),
            )
            for k in range(1, 4)
            for w in range(2)
        ] + [remote(e_part.at[ch, y, o], e_recv.at[ch, 6], es_s.at[1], es_r.at[ch], partner)]

    def combine(ch, _):
        @pl.when(par == o)
        def _():
            await_recv(back.at[ch, 0:15], r_r.at[ch])

        @pl.when(par != o)
        def _():
            await_recv(back.at[ch], r_r.at[ch])

        returned = back[ch].reshape(768, CW)
        e_part[ch] = e_part[ch] + (
            dot(mix_hi[...], returned) + dot(mix_lo[...], returned)
        ).reshape(4, 2, 32, CW)
        for copy in final(ch):
            copy.start()
        return 0

    lax.fori_loop(0, NCH // 2, combine, 0)
    settle(m_part, m_send, m_recv, m_sum, m_other, ms_s, ms_r, 0)
    finish(m_sum, m_other, mscale, out_m, 0)
    lax.fori_loop(NCH // 2, NCH, combine, 0)
    await_send(send_x, d_s.at[0])
    await_send(send_n, d_s.at[1])
    await_send(rows.at[0:2, 0:FAR], f_s.at[0])
    await_send(carries, c_s.at[0])

    @pl.when(par == o)
    def _():
        for ch in range(NCH):
            await_send(back.at[ch, 0:15], r_s.at[ch])

    @pl.when(par != o)
    def _():
        for ch in range(NCH):
            await_send(back.at[ch], r_s.at[ch])

    await_send(m_recv, ms_s.at[0])
    await_send(m_other, x_s.at[0])
    for copy in swaps:
        copy.wait_send()
    give_halo.wait_send()

    def settle_last(ch, square):
        await_recv(e_recv.at[ch, 0:7], es_r.at[ch])
        mine = e_part[ch, y, c] + e_recv[ch, c] + e_recv[ch, 2 + c] + e_recv[ch, 4 + c]
        theirs = e_recv[ch, 6] + e_recv[ch, o] + e_recv[ch, 2 + o] + e_recv[ch, 4 + o]
        e_sum[ch, c] = mine
        e_sum[ch, o] = theirs
        return square + jnp.sum(mine * mine + theirs * theirs, axis=1, keepdims=True)

    square = lax.fori_loop(0, NCH, settle_last, jnp.zeros((32, 1), f32))
    level = lax.rsqrt(square / 4096.0 + eps)
    for ch in range(NCH):
        for w in range(2):
            cols = slice(w * 2048 + ch * CW, w * 2048 + ch * CW + CW)
            out_e[:, cols] = (e_sum[ch, w] * level * escale[:, cols]).astype(bf16)

    await_send(e_part.at[:, 1:4], es_s.at[0])
    await_send(e_part.at[:, 0, 0], es_s.at[1])


def body(
    mixer_rows, mixer_gain, gate_proj, input_proj, conv_taps, input_gates, decay_gates,
    decay_offset, out_proj, mixer_scale, expert_rows, expert_gain, route_ids, route_weights,
    expert_gate, expert_up, expert_down, shared_gate, shared_up, shared_down, expert_scale,
):
    f32, bf16 = jnp.float32, jnp.bfloat16
    dma = pltpu.SemaphoreType.DMA
    hbm = pl.BlockSpec(memory_space=pltpu.HBM)
    vmem = pl.BlockSpec(memory_space=pltpu.VMEM)
    outs = pl.pallas_call(
        whole_kernel,
        out_shape=[jax.ShapeDtypeStruct((32, 4096), bf16)] * 2,
        in_specs=[hbm] * 21,
        out_specs=[vmem] * 2,
        scratch_shapes=[
            pltpu.VMEM((1, 4096), f32),
            pltpu.VMEM((4, 512), f32),
            pltpu.VMEM((1, 512), f32),
            pltpu.VMEM((1, 4096), f32),
            pltpu.VMEM((1, 4096), f32),
            pltpu.VMEM((2, 256), jnp.int32),
            pltpu.VMEM((2, 256), f32),
            pltpu.VMEM((1, 4096), f32),
            pltpu.VMEM((4, 256, 1024), bf16),
            pltpu.VMEM((256, 4096), bf16),
            pltpu.VMEM((2, 4096, 512), bf16),
            pltpu.VMEM((2, 2, 256, 256), bf16),
            pltpu.VMEM((2, 8, 48, 1024), bf16),
            pltpu.VMEM((2, 8 - FAR, 48, 1024), bf16),
            pltpu.VMEM((4096, 256), bf16),
            pltpu.VMEM((256, 512), bf16),
            pltpu.VMEM((16, 4096), bf16),
            pltpu.VMEM((16, 512), bf16),
            pltpu.VMEM((16, 512), bf16),
            pltpu.VMEM((256, 512), f32),
            pltpu.VMEM((256, 512), f32),
            pltpu.VMEM((256, 512), f32),
            pltpu.VMEM((8, 128), f32),
            pltpu.VMEM((256, 128), bf16),
            pltpu.VMEM((256, 768), bf16),
            pltpu.VMEM((256, 768), bf16),
            pltpu.VMEM((4, 8, 48, 1024), bf16),
            pltpu.VMEM((4096, 512), bf16),
            pltpu.VMEM((256, 4096), bf16),
            pltpu.VMEM((2, 128, 2048), bf16),
            pltpu.VMEM((2, 512, 2048), bf16),
            pltpu.VMEM((256, 128), bf16),
            pltpu.VMEM((2, 256, 512), bf16),
            pltpu.VMEM((15, 8, 128), f32),
            pltpu.VMEM((384, 512), f32),
            pltpu.VMEM((384, 256), bf16),
            pltpu.VMEM((NCH, 2, 8, 48, CW), bf16),
            pltpu.VMEM((NCH, 16, 48, CW), bf16),
        ]
        + [
            pltpu.VMEM((NCH, 4, 64, CW), f32),
            pltpu.VMEM((NCH, 4, 64, CW), bf16),
            pltpu.VMEM((NCH, 3, 64, CW), bf16),
            pltpu.VMEM((NCH, 2, 32, CW), f32),
            pltpu.VMEM((NCH, 32, CW), f32),
            pltpu.VMEM((NCH, 4, 2, 32, CW), f32),
            pltpu.VMEM((NCH, 7, 32, CW), f32),
            pltpu.VMEM((NCH, 2, 32, CW), f32),
        ]
        + [
            dma((2,)), dma((FAR + 5,)), dma((1,)), dma((2, 2)), dma((1,)), dma((1,)),
            dma((7,)), dma((7,)), dma((23,)), dma((NCH,)), dma((NCH,)),
            dma((1,)), dma((1,)), dma((2,)), dma((NCH,)), dma((1,)), dma((1,)), dma((1,)), dma((1,)),
        ],
        compiler_params=pltpu.CompilerParams(
            collective_id=0, has_side_effects=True, vmem_limit_bytes=67043328
        ),
    )(
        mixer_rows, gate_proj, input_proj, input_gates, decay_gates, out_proj, expert_rows,
        expert_gate[0], expert_up[0], expert_down[0], shared_gate, shared_up, shared_down,
        mixer_gain[None, :], conv_taps, decay_offset[None, :], mixer_scale[None, :],
        expert_gain[None, :], route_ids.T, route_weights.T, expert_scale[None, :],
    )

    def hand_out(a, b, a_out, b_out):
        a_out[...] = a[...]
        b_out[...] = b[...]

    return tuple(
        pl.pallas_call(
            hand_out,
            out_shape=[jax.ShapeDtypeStruct((32, 4096), bf16)] * 2,
            in_specs=[vmem] * 2,
            out_specs=[vmem] * 2,
        )(*outs)
    )


def solution(mesh):
    placed = (
        P("ep", None),
        P(),
        P(None, "tp"),
        P(None, "tp"),
        P(None, "tp"),
        P("tp", None, None),
        P("tp", None, None),
        P("tp"),
        P("tp", None),
        P(),
        P("ep", None),
        P(),
        P("ep", None),
        P("ep", None),
        P("ep", None, "tp"),
        P("ep", None, "tp"),
        P("ep", "tp", None),
        P(None, "tp"),
        P(None, "tp"),
        P("tp", None),
        P(),
    )
    return jax.shard_map(
        body,
        mesh=mesh,
        in_specs=placed,
        out_specs=(P(("ep", "tp"), None), P(("ep", "tp"), None)),
        check_vma=False,
    )
```

```python
import jax
import jax.numpy as jnp
from jax import lax
from jax.experimental import pallas as pl
from jax.experimental.pallas import tpu as pltpu
from jax.sharding import PartitionSpec as P

eps = 1e-06
lru_power = 8.0


MESH = pl.DeviceIdType.MESH
NCH = 4
FAR = 7
LEAD = 1
CW = 2048 // NCH
FAR_EVEN = ((2, 2), (1, 2), (3, 2), (2, 0), (0, 2), (1, 0), (3, 0), (0, 0))
FAR_ODD = ((2, 1), (2, 3), (1, 1), (3, 3), (1, 3), (3, 1), (0, 1), (0, 3))


def remote(src, dst, send, recv, device):
    return pltpu.make_async_remote_copy(
        src_ref=src, dst_ref=dst, send_sem=send, recv_sem=recv, device_id=device, device_id_type=MESH
    )


def hop(step, even, core):
    dz = jnp.where(even, FAR_EVEN[step][0], FAR_ODD[step][0])
    dx = jnp.where(even, FAR_EVEN[step][1], FAR_ODD[step][1])
    return jnp.where(core == 0, dz, (4 - dz) % 4), jnp.where(core == 0, dx, (4 - dx) % 4)


def log1p_small(u):
    series = u * (1 - u * (1 / 2 - u * (1 / 3 - u * (1 / 4 - u * (1 / 5 - u * (1 / 6))))))
    return jnp.where(u < 0.05, series, jnp.log(1.0 + u))


def one_minus_exp(z):
    series = 1.0 + z * (1 / 7)
    for n in (6, 5, 4, 3, 2):
        series = 1.0 + z * series * (1 / n)
    return jnp.where(z > -0.5, -z * series, 1.0 - jnp.exp(z))


def sigmoid(v):
    return 1.0 / (1.0 + jnp.exp(-v))


def whole_kernel(
    m_rows, g_proj, i_proj, i_gates, d_gates, op, x_rows, eg, eu, ed, sg, su, sd,
    m_gain_h, taps_h, offset_h, mscale_h, x_gain_h, ids_h, weights_h, escale_h,
    out_m, out_e,
    m_gain, taps, offset, mscale, x_gain, ids, weights, escale,
    nx, nm, proj, bgates, send_x, send_n, w_sh, br, tail, edge, halo, gate, acum, loc, cm, sh, mix_hi, mix_lo,
    rows, w_in, w_dn, s_dn, o_pr, sh2, gts, carries, acc, hid, res, back,
    m_part, m_send, m_recv, m_sum, m_other, e_part, e_recv, e_sum,
    d_s, d_r, f_s, f_r, c_s, c_r, p_s, p_r, l_s, r_s, r_r, ms_s, ms_r, es_s, es_r, x_s, x_r, h_s, h_r,
):
    f32, bf16 = jnp.float32, jnp.bfloat16
    p = lax.axis_index("ep")
    t = lax.axis_index("tp")
    y = t // 2
    c = t % 2
    o = 1 - c
    z = p // 4
    x = p % 4
    par = p % 2
    half = p // 2
    partner = (p, 2 * y + o)

    def dot(a, b):
        return jnp.dot(a, b, preferred_element_type=f32)

    def wide(at):
        return pl.ds(pl.multiple_of(at * 2048, 2048), 2048)

    def local(src, dst, n):
        return pltpu.make_async_copy(src, dst, l_s.at[n])

    early = [local(m_rows.at[240:256], tail, 1), local(i_proj, proj.at[1], 2)]
    first = [
        local(
            x_rows.at[r : r + 128, 1024 * q : 1024 * q + 1024], nx.at[q, r : r + 128], 22 if r else 0
        )
        for r in (0, 128)
        for q in range(4)
    ]
    second = [local(m_rows, nm, 3), local(g_proj, proj.at[0], 4)]
    gates_in = [local(i_gates, bgates.at[0], 5), local(d_gates, bgates.at[1], 6)]
    own_w = [
        local(eg, w_in.at[:, 0:128], 7),
        local(eu, w_in.at[:, 128:256], 8),
        local(ed, w_dn.at[0:128], 9),
    ]
    own_o = local(op.at[:, wide(c)], o_pr.at[0], 10)
    own_s = [
        local(sd.at[:, wide(c)], s_dn.at[0], 11),
        local(sg, w_sh.at[:, 0:128], 12),
        local(su, w_sh.at[:, 128:256], 13),
    ]
    small = [local(ids_h, ids, 14), local(weights_h, weights, 15), local(x_gain_h, x_gain, 16)]
    small += [local(m_gain_h, m_gain, 17), local(taps_h, taps, 18), local(offset_h, offset, 19)]
    small += [local(mscale_h, mscale, 20), local(escale_h, escale, 21)]
    for copy in small[:1] + first + small[1:]:
        copy.start()

    barrier = pltpu.get_barrier_semaphore()

    for k in range(1, 32):
        other = lax.rem(p * 2 + c + k, 32)
        pl.semaphore_signal(
            barrier, inc=1, device_id=(lax.div(other, 2), 2 * y + lax.rem(other, 2)), device_id_type=MESH
        )
    for k in range(1, 4):
        pl.semaphore_signal(
            barrier, inc=1, device_id=(p, 2 * ((y + k) % 4) + c), device_id_type=MESH
        )

    small[0].wait()

    def await_recv(group, sem):
        remote(group, group, h_s.at[0], sem, partner).wait_recv()

    def await_send(group, sem):
        remote(group, group, sem, h_r.at[0], partner).wait_send()

    id0, id1 = ids[0:1, :], ids[1:2, :]
    expert = lax.broadcasted_iota(jnp.int32, (16, 256), 0)
    named0, named1 = id0 == expert, id1 == expert
    either = jnp.where(jnp.logical_or(named0, named1), 1.0, 0.0).astype(bf16)
    ahead = jnp.where(
        lax.broadcasted_iota(jnp.int32, (256, 256), 0) < lax.broadcasted_iota(jnp.int32, (256, 256), 1),
        1.0,
        0.0,
    ).astype(bf16)
    place = dot(either, ahead)
    slot0 = id0.astype(f32) * 48.0 + jnp.sum(jnp.where(named0, place, 0.0), axis=0, keepdims=True)
    slot1 = id1.astype(f32) * 48.0 + jnp.sum(jnp.where(named1, place, 0.0), axis=0, keepdims=True)

    def picked(i):
        line = ((2 * i + c) * 48 + lax.broadcasted_iota(jnp.int32, (48, 256), 0)).astype(f32)
        return jnp.where(jnp.logical_or(slot0 == line, slot1 == line), 1.0, 0.0).astype(bf16)

    chosen = jnp.concatenate([picked(i) for i in range(8)], axis=0)

    for copy in small[1:]:
        copy.wait()

    def norm_x(r, _):
        at = pl.ds(pl.multiple_of(r * 32, 32), 32)
        parts = [nx[q, at, :].astype(f32) for q in range(4)]
        square = sum(jnp.sum(v * v, axis=1, keepdims=True) for v in parts)
        scale = lax.rsqrt(square / 4096.0 + eps)
        for q in range(4):
            nx[q, at, :] = (parts[q] * scale * x_gain[:, 1024 * q : 1024 * q + 1024]).astype(bf16)
        return 0

    def dispatch(step, j):
        dz, dx = hop(step, par == c, c)
        e = ((z + dz) % 4) * 4 + (x + dx) % 4
        source = send_x.at[j, e // 2] if j < 2 else send_n.at[j - 2, step - FAR]
        shift = (0, 2, 1, 3)[j]
        return remote(
            source, rows.at[(y + shift) % 4, step], d_s.at[j // 2], d_r.at[landing(step, j)],
            (e, 2 * y + 1 - par),
        )

    def landing(step, j):
        if j == 0:
            return min(step, FAR)
        return FAR + (1 + step // 4 if j == 1 else 1 + j)

    def group(low, high, j):
        shift = (0, 2, 1, 3)[j]
        await_recv(rows.at[(y + shift) % 4, low:high], d_r.at[landing(low, j)])

    def gather(j):
        send_x[j] = dot(chosen, nx[(y + 2 * j) % 4]).astype(bf16).reshape(8, 48, 1024)

    local(nx.at[:, 0:128], nx.at[:, 0:128], 0).wait()
    lax.fori_loop(0, 4, norm_x, 0)
    local(nx.at[:, 128:256], nx.at[:, 128:256], 22).wait()
    for copy in early + second + gates_in:
        copy.start()
    lax.fori_loop(4, 8, norm_x, 0)
    gather(0)
    pl.semaphore_wait(barrier, 34)
    for step in range(4):
        dispatch(step, 0).start()
    gather(1)
    for step in range(4):
        dispatch(step, 1).start()

    for copy in early:
        copy.wait()
    v = tail[...].astype(f32)
    tail_factor = lax.rsqrt(jnp.sum(v * v, axis=1, keepdims=True) / 4096.0 + eps)
    edge[...] = dot((v * tail_factor * m_gain[...]).astype(bf16), proj[1]).astype(bf16)
    give_halo = remote(edge, halo, h_s.at[0], h_r.at[0], ((p + 1) % 16, t))
    give_halo.start()
    for j in range(2):
        for step in range(4, FAR):
            dispatch(step, j).start()

    near = []
    for step in range(FAR, 8):
        dz, dx = hop(step, par == c, c)
        near.append((((z + dz) % 4) * 4 + (x + dx) % 4) // 2)
    near_chosen = jnp.concatenate([picked(i) for i in near], axis=0)
    for j in range(2):
        send_n[j] = dot(near_chosen, nx[(y + 1 + 2 * j) % 4]).astype(bf16).reshape(8 - FAR, 48, 1024)
    for j in range(4):
        for step in range(FAR, 8):
            dispatch(step, j).start()

    swaps = [
        remote(sh, sh2, p_s.at[0], p_r.at[0], partner),
        remote(op.at[:, wide(o)], o_pr.at[1], p_s.at[1], p_r.at[1], partner),
        remote(eg, w_in.at[:, 256:384], p_s.at[2], p_r.at[2], partner),
        remote(eu, w_in.at[:, 384:512], p_s.at[3], p_r.at[3], partner),
        remote(ed, w_dn.at[128:256], p_s.at[4], p_r.at[4], partner),
        remote(sd.at[:, wide(o)], s_dn.at[1], p_s.at[5], p_r.at[5], partner),
        remote(gts.at[0], gts.at[1], p_s.at[6], p_r.at[6], partner),
    ]
    for copy in swaps[2:5] + own_w + [swaps[1], own_o, swaps[5]] + own_s:
        copy.start()

    def forward(i, d):
        return remote(
            rows.at[y, i], rows.at[y, i], f_s.at[0], f_r.at[i // 4, d],
            (p, 2 * ((y + 1 + 2 * d) % 4) + c),
        )

    def relay(step):
        group(step, step + 1, 0)
        forward(step, 0).start()
        forward(step, 1).start()

    second[0].wait()

    def norm_m(r, _):
        at = pl.ds(pl.multiple_of(r * 32, 32), 32)
        v = nm[at, :].astype(f32)
        scale = lax.rsqrt(jnp.sum(v * v, axis=1, keepdims=True) / 4096.0 + eps)
        nm[at, :] = (v * scale * m_gain[...]).astype(bf16)
        return 0

    lax.fori_loop(0, 8, norm_m, 0)

    def project(n, _):
        cols = pl.ds(pl.multiple_of(n * 256, 256), 256)
        br[:, cols] = dot(nm[...], proj[1, :, cols]).astype(bf16)
        return 0

    lax.fori_loop(0, 2, project, 0)
    second[1].wait()

    def gates(n, _):
        cols = pl.ds(pl.multiple_of(n * 256, 256), 256)
        v = dot(nm[...], proj[0, :, cols])
        gate[:, cols] = 0.5 * v * (1.0 + jnp.tanh(0.7978845608028654 * (v + 0.044715 * (v * v * v))))
        return 0

    relay(0)
    relay(1)
    gates(0, 0)
    relay(2)
    gates(1, 0)
    relay(3)
    for copy in gates_in:
        copy.wait()
    give_halo.wait_recv()

    row = lax.broadcasted_iota(jnp.int32, (256, 128), 0)

    def recur(b, _):
        cols = pl.ds(pl.multiple_of(b * 256, 256), 256)
        before = jnp.where(p == 0, 0.0, halo[:, cols].astype(f32))
        ext = jnp.concatenate([before, br[:, cols].astype(f32)], axis=0)
        tap = taps[:, cols]
        conv = tap[0:1] * pltpu.roll(ext, 3, 0)[16:]
        for k in range(1, 4):
            conv = conv + tap[k : k + 1] * (pltpu.roll(ext, 3 - k, 0) if k < 3 else ext)[16:]
        conv_out = conv.astype(bf16)
        gi = sigmoid(dot(conv_out, bgates[0, b]))
        gd = sigmoid(dot(conv_out, bgates[1, b]))
        off = offset[:, cols]
        soft = jnp.maximum(-off, 0.0) + log1p_small(jnp.exp(-jnp.abs(off)))
        log_decay = -lru_power * gd * soft
        scale = jnp.sqrt(one_minus_exp(2.0 * log_decay))
        first_row = jnp.logical_and(lax.broadcasted_iota(jnp.int32, (256, 256), 0) == 0, p == 0)
        scale = jnp.where(first_row, 1.0, scale)
        loc[:, cols] = scale * gi * conv_out.astype(f32)
        acum[:, cols] = jnp.exp(log_decay)
        return 0

    recur(0, 0)
    relay(4)
    recur(1, 0)
    relay(5)
    relay(6)

    def scan(b, _):
        cols = pl.ds(pl.multiple_of(b * 128, 128), 128)
        av, bv = acum[:, cols], loc[:, cols]
        for d in (1, 2, 4, 8, 16, 32, 64, 128):
            if d < 8:
                a_up = jnp.where(row < d, 1.0, pltpu.roll(av, d, 0))
                b_up = jnp.where(row < d, 0.0, pltpu.roll(bv, d, 0))
            else:
                a_up = jnp.concatenate([jnp.ones((d, 128), f32), av[: 256 - d]], axis=0)
                b_up = jnp.concatenate([jnp.zeros((d, 128), f32), bv[: 256 - d]], axis=0)
            bv = av * b_up + bv
            av = av * a_up
        acum[:, cols] = av
        loc[:, cols] = bv
        cm[pl.ds(b, 1), :] = av[255:256]
        cm[pl.ds(4 + b, 1), :] = bv[255:256]
        return 0

    lax.fori_loop(0, 4, scan, 0)

    def carry(k):
        return remote(cm, carries.at[k - 1], c_s.at[0], c_r.at[0], ((p + k) % 16, t))

    def carry_go(k, _):
        carry(k).start()
        return 0

    lax.fori_loop(1, 16, carry_go, 0)
    line = lax.broadcasted_iota(jnp.int32, (128, 256), 0)
    tile = jnp.where(
        line == 0, slot0,
        jnp.where(line == 1, slot1, jnp.where(line == 2, weights[0:1, :], jnp.where(line == 3, weights[1:2, :], 0.0))),
    )
    turned = tile.T
    every = lax.broadcasted_iota(jnp.int32, (256, 768), 1).astype(f32)
    mixing = jnp.where(turned[:, 0:1] == every, turned[:, 2:3], 0.0) + jnp.where(
        turned[:, 1:2] == every, turned[:, 3:4], 0.0
    )
    high = mixing.astype(bf16)
    mix_hi[...] = high
    mix_lo[...] = (mixing - high.astype(f32)).astype(bf16)

    def scatter(part, recv, send_sem, recv_sem, ch):
        return [
            remote(
                part.at[ch, (y + k) % 4], recv.at[ch, k - 1], send_sem.at[0],
                recv_sem.at[0], (p, 2 * ((y + k) % 4) + c),
            )
            for k in range(1, 4)
        ]

    def swap(total, other, base, ch):
        return remote(
            total.at[ch, o], other.at[ch], x_s.at[0], x_r.at[0], partner
        )

    def settle(part, sent, recv, total, other, send_sem, recv_sem, base):
        await_recv(recv, recv_sem.at[0])

        def one(ch, _):
            value = part[ch, y] + sum(recv[ch, k].astype(f32) for k in range(3))
            total[ch] = value.reshape(2, 32, CW)
            swap(total, other, base, ch).start()
            return 0

        lax.fori_loop(0, NCH, one, 0)

    def finish(total, other, scale, out, base):
        square = jnp.zeros((32, 1), f32)
        await_recv(other, x_r.at[0])
        for ch in range(NCH):
            mine, theirs = total[ch, c], other[ch]
            square += jnp.sum(mine * mine + theirs * theirs, axis=1, keepdims=True)
        level = lax.rsqrt(square / 4096.0 + eps)
        for ch in range(NCH):
            for values, side in ((total[ch, c], c), (other[ch], o)):
                cols = pl.ds(pl.multiple_of(side * 2048 + ch * CW, CW), CW)
                out[:, cols] = (values * level * scale[:, cols]).astype(bf16)

    for copy in own_w:
        copy.wait()
    for copy in swaps[2:5]:
        copy.wait_recv()

    def hidden(half_of):
        at = slice(192 * half_of, 192 * half_of + 192)

        def quarter(q):
            depth = pl.ds(pl.multiple_of(q * 1024, 1024), 1024)
            block = rows[q, 4 * half_of : 4 * half_of + 4].reshape(192, 1024)
            return dot(block, w_in[depth, :])

        if half_of == 1:
            group(FAR, 8, 0)
        acc[at] = quarter(y)
        group(4 * half_of, 4 * half_of + 4, 1)
        acc[at] += quarter((y + 2) % 4)
        for d in range(2):
            source = (y + 3 + 2 * d) % 4
            await_recv(rows.at[source, 4 * half_of : min(FAR, 4 * half_of + 4)], f_r.at[half_of, d])
            if half_of == 1:
                group(FAR, 8, 3 - d)
            acc[at] += quarter(source)
        for side in range(2):
            g = acc[at, 256 * side : 256 * side + 128]
            u = acc[at, 256 * side + 128 : 256 * side + 256]
            hid[at, 128 * side : 128 * side + 128] = (g / (1.0 + jnp.exp(-g)) * u).astype(bf16)

    def returning(ch, step, h):
        dz, dx = hop(step, par == o, par)
        s = ((z + 4 - dz) % 4) * 4 + (x + 4 - dx) % 4
        return s, remote(
            res.at[ch, h, step], back.at[ch, p], r_s.at[ch], r_r.at[ch], (s, 2 * y + h)
        )

    def give(low, high):
        def one(ch, _):
            for h in range(2):
                cols = pl.ds(pl.multiple_of(h * 2048 + ch * CW, CW), CW)
                res[ch, h, low:high] = (
                    dot(hid[48 * low : 48 * high], w_dn[:, cols]).astype(bf16).reshape(high - low, 48, CW)
                )
            for h in range(2):
                for step in range(low, high):
                    s, copy = returning(ch, step, h)
                    if step < 7:
                        copy.start()
                    else:

                        @pl.when(jnp.logical_or(s != p, c != h))
                        def _():
                            copy.start()

                        @pl.when(jnp.logical_and(s == p, c == h))
                        def _():
                            back[ch, p] = res[ch, h, step]

            return 0

        return one

    hidden(0)
    lax.fori_loop(0, LEAD, give(0, 4), 0)
    hidden(1)
    lax.fori_loop(0, LEAD, give(4, 8), 0)
    lax.fori_loop(LEAD, NCH, give(0, 8), 0)

    await_recv(carries, c_r.at[0])

    def fold(n, state):
        k = 15 - n
        later = carries[k - 1]
        return jnp.where(k <= p, later[0:4] * state + later[4:8], state)

    state = lax.fori_loop(0, 15, fold, jnp.zeros((4, 128), f32))
    for j in range(4):
        cols = slice(128 * j, 128 * j + 128)
        states = loc[:, cols] + acum[:, cols] * state[j : j + 1]
        gts[0, :, cols] = (gate[:, cols] * states).astype(bf16)

    swaps[6].start()

    for copy in own_s:
        copy.wait()
    shared = dot(nx[0], w_sh[0:1024, :])
    for q in range(1, 4):
        shared = shared + dot(nx[q], w_sh[1024 * q : 1024 * q + 1024, :])
    g, u = shared[:, 0:128], shared[:, 128:256]
    sh[...] = (g / (1.0 + jnp.exp(-g)) * u).astype(bf16)
    swaps[0].start()

    own_o.wait()
    swaps[1].wait_recv()
    swaps[6].wait_recv()

    def mixed(ch, _):
        cols = pl.ds(pl.multiple_of(ch * CW, CW), CW)
        m_part[ch] = (dot(gts[0], o_pr[0, :, cols]) + dot(gts[1], o_pr[1, :, cols])).reshape(4, 64, CW)
        m_send[ch] = m_part[ch].astype(bf16)
        for copy in scatter(m_send, m_recv, ms_s, ms_r, ch):
            copy.start()
        return 0

    lax.fori_loop(0, NCH, mixed, 0)

    swaps[0].wait_recv()
    swaps[5].wait_recv()

    def shared_part(ch, _):
        cols = pl.ds(pl.multiple_of(ch * CW, CW), CW)
        e_part[ch] = (dot(sh[...], s_dn[0, :, cols]) + dot(sh2[...], s_dn[1, :, cols])).reshape(4, 2, 32, CW)
        return 0

    lax.fori_loop(0, NCH, shared_part, 0)

    def final(ch):
        return [
            remote(
                e_part.at[ch, (y + k) % 4, w], e_recv.at[ch, 2 * (k - 1) + c], es_s.at[0],
                es_r.at[ch], (p, 2 * ((y + k) % 4) + w),
            )
            for k in range(1, 4)
            for w in range(2)
        ] + [remote(e_part.at[ch, y, o], e_recv.at[ch, 6], es_s.at[1], es_r.at[ch], partner)]

    def combine(ch, _):
        @pl.when(par == o)
        def _():
            await_recv(back.at[ch, 0:15], r_r.at[ch])

        @pl.when(par != o)
        def _():
            await_recv(back.at[ch], r_r.at[ch])

        returned = back[ch].reshape(768, CW)
        e_part[ch] = e_part[ch] + (
            dot(mix_hi[...], returned) + dot(mix_lo[...], returned)
        ).reshape(4, 2, 32, CW)
        for copy in final(ch):
            copy.start()
        return 0

    lax.fori_loop(0, NCH // 2, combine, 0)
    settle(m_part, m_send, m_recv, m_sum, m_other, ms_s, ms_r, 0)
    finish(m_sum, m_other, mscale, out_m, 0)
    lax.fori_loop(NCH // 2, NCH, combine, 0)
    await_send(send_x, d_s.at[0])
    await_send(send_n, d_s.at[1])
    await_send(rows.at[0:2, 0:FAR], f_s.at[0])
    await_send(carries, c_s.at[0])

    @pl.when(par == o)
    def _():
        for ch in range(NCH):
            await_send(back.at[ch, 0:15], r_s.at[ch])

    @pl.when(par != o)
    def _():
        for ch in range(NCH):
            await_send(back.at[ch], r_s.at[ch])

    await_send(m_recv, ms_s.at[0])
    await_send(m_other, x_s.at[0])
    for copy in swaps:
        copy.wait_send()
    give_halo.wait_send()

    def settle_last(ch, square):
        await_recv(e_recv.at[ch, 0:7], es_r.at[ch])
        mine = e_part[ch, y, c] + e_recv[ch, c] + e_recv[ch, 2 + c] + e_recv[ch, 4 + c]
        theirs = e_recv[ch, 6] + e_recv[ch, o] + e_recv[ch, 2 + o] + e_recv[ch, 4 + o]
        e_sum[ch, c] = mine
        e_sum[ch, o] = theirs
        return square + jnp.sum(mine * mine + theirs * theirs, axis=1, keepdims=True)

    square = lax.fori_loop(0, NCH, settle_last, jnp.zeros((32, 1), f32))
    level = lax.rsqrt(square / 4096.0 + eps)
    for ch in range(NCH):
        for w in range(2):
            cols = slice(w * 2048 + ch * CW, w * 2048 + ch * CW + CW)
            out_e[:, cols] = (e_sum[ch, w] * level * escale[:, cols]).astype(bf16)

    await_send(e_part.at[:, 1:4], es_s.at[0])
    await_send(e_part.at[:, 0, 0], es_s.at[1])


def body(
    mixer_rows, mixer_gain, gate_proj, input_proj, conv_taps, input_gates, decay_gates,
    decay_offset, out_proj, mixer_scale, expert_rows, expert_gain, route_ids, route_weights,
    expert_gate, expert_up, expert_down, shared_gate, shared_up, shared_down, expert_scale,
):
    f32, bf16 = jnp.float32, jnp.bfloat16
    dma = pltpu.SemaphoreType.DMA
    hbm = pl.BlockSpec(memory_space=pltpu.HBM)
    vmem = pl.BlockSpec(memory_space=pltpu.VMEM)
    outs = pl.pallas_call(
        whole_kernel,
        out_shape=[jax.ShapeDtypeStruct((32, 4096), bf16)] * 2,
        in_specs=[hbm] * 21,
        out_specs=[vmem] * 2,
        scratch_shapes=[
            pltpu.VMEM((1, 4096), f32),
            pltpu.VMEM((4, 512), f32),
            pltpu.VMEM((1, 512), f32),
            pltpu.VMEM((1, 4096), f32),
            pltpu.VMEM((1, 4096), f32),
            pltpu.VMEM((2, 256), jnp.int32),
            pltpu.VMEM((2, 256), f32),
            pltpu.VMEM((1, 4096), f32),
            pltpu.VMEM((4, 256, 1024), bf16),
            pltpu.VMEM((256, 4096), bf16),
            pltpu.VMEM((2, 4096, 512), bf16),
            pltpu.VMEM((2, 2, 256, 256), bf16),
            pltpu.VMEM((2, 8, 48, 1024), bf16),
            pltpu.VMEM((2, 8 - FAR, 48, 1024), bf16),
            pltpu.VMEM((4096, 256), bf16),
            pltpu.VMEM((256, 512), bf16),
            pltpu.VMEM((16, 4096), bf16),
            pltpu.VMEM((16, 512), bf16),
            pltpu.VMEM((16, 512), bf16),
            pltpu.VMEM((256, 512), f32),
            pltpu.VMEM((256, 512), f32),
            pltpu.VMEM((256, 512), f32),
            pltpu.VMEM((8, 128), f32),
            pltpu.VMEM((256, 128), bf16),
            pltpu.VMEM((256, 768), bf16),
            pltpu.VMEM((256, 768), bf16),
            pltpu.VMEM((4, 8, 48, 1024), bf16),
            pltpu.VMEM((4096, 512), bf16),
            pltpu.VMEM((256, 4096), bf16),
            pltpu.VMEM((2, 128, 2048), bf16),
            pltpu.VMEM((2, 512, 2048), bf16),
            pltpu.VMEM((256, 128), bf16),
            pltpu.VMEM((2, 256, 512), bf16),
            pltpu.VMEM((15, 8, 128), f32),
            pltpu.VMEM((384, 512), f32),
            pltpu.VMEM((384, 256), bf16),
            pltpu.VMEM((NCH, 2, 8, 48, CW), bf16),
            pltpu.VMEM((NCH, 16, 48, CW), bf16),
        ]
        + [
            pltpu.VMEM((NCH, 4, 64, CW), f32),
            pltpu.VMEM((NCH, 4, 64, CW), bf16),
            pltpu.VMEM((NCH, 3, 64, CW), bf16),
            pltpu.VMEM((NCH, 2, 32, CW), f32),
            pltpu.VMEM((NCH, 32, CW), f32),
            pltpu.VMEM((NCH, 4, 2, 32, CW), f32),
            pltpu.VMEM((NCH, 7, 32, CW), f32),
            pltpu.VMEM((NCH, 2, 32, CW), f32),
        ]
        + [
            dma((2,)), dma((FAR + 5,)), dma((1,)), dma((2, 2)), dma((1,)), dma((1,)),
            dma((7,)), dma((7,)), dma((23,)), dma((NCH,)), dma((NCH,)),
            dma((1,)), dma((1,)), dma((2,)), dma((NCH,)), dma((1,)), dma((1,)), dma((1,)), dma((1,)),
        ],
        compiler_params=pltpu.CompilerParams(
            collective_id=0, has_side_effects=True, vmem_limit_bytes=67043328
        ),
    )(
        mixer_rows, gate_proj, input_proj, input_gates, decay_gates, out_proj, expert_rows,
        expert_gate[0], expert_up[0], expert_down[0], shared_gate, shared_up, shared_down,
        mixer_gain[None, :], conv_taps, decay_offset[None, :], mixer_scale[None, :],
        expert_gain[None, :], route_ids.T, route_weights.T, expert_scale[None, :],
    )

    def hand_out(a, b, a_out, b_out):
        a_out[...] = a[...]
        b_out[...] = b[...]

    return tuple(
        pl.pallas_call(
            hand_out,
            out_shape=[jax.ShapeDtypeStruct((32, 4096), bf16)] * 2,
            in_specs=[vmem] * 2,
            out_specs=[vmem] * 2,
        )(*outs)
    )


def solution(mesh):
    placed = (
        P("ep", None),
        P(),
        P(None, "tp"),
        P(None, "tp"),
        P(None, "tp"),
        P("tp", None, None),
        P("tp", None, None),
        P("tp"),
        P("tp", None),
        P(),
        P("ep", None),
        P(),
        P("ep", None),
        P("ep", None),
        P("ep", None, "tp"),
        P("ep", None, "tp"),
        P("ep", "tp", None),
        P(None, "tp"),
        P(None, "tp"),
        P("tp", None),
        P(),
    )
    return jax.shard_map(
        body,
        mesh=mesh,
        in_specs=placed,
        out_specs=(P(("ep", "tp"), None), P(("ep", "tp"), None)),
        check_vma=False,
    )
```
